512 devices in a mesh: rep: 64 (over z, y), fs: 4 (over x), tp: 2 (over core).
Axes of the slice: x: 4, y: 8, z: 8, core: 2. Of those that a mesh axis runs over, the one named last changes fastest.
Arguments:
- gate_pre: bfloat16 [40960, 2816], P(('rep', 'fs'), 'tp'), may hold values from -6 to 6
- up_pre: bfloat16 [40960, 2816], P(('rep', 'fs'), 'tp'), may hold values from -6 to 6
- gate_taps: bfloat16 [3, 2816], P(None, 'tp'), may hold values from -3 to 3
- up_taps: bfloat16 [3, 2816], P(None, 'tp'), may hold values from -3 to 3
- down_weight: bfloat16 [2816, 2048], P('tp', 'fs'), may hold values from -0.125 to 0.125
- cotangent: bfloat16 [40960, 2048], P('rep', 'fs'), may hold values from -16 to 16
Outputs:
- grad_gate: bfloat16 [40960, 2816], P(('rep', 'fs'), 'tp')
- grad_up: bfloat16 [40960, 2816], P(('rep', 'fs'), 'tp')
- grad_gate_taps: float32 [3, 2816], P(None, 'tp')
- grad_up_taps: float32 [3, 2816], P(None, 'tp')
- grad_down: float32 [4, 512, 2816], P('fs', 'rep', 'tp')
- down_norms: float32 [2816], P('tp')
The draws below stay inside these ranges and needn't reach their ends.
All inputs are finite; a program needn't handle non-finite values.
Results may differ from the reference program's by a relative error of at most 0.0049.
Values may be sent and summed in bfloat16 or wider, within the bound.
No kernel may reach another device: no remote copies, remote signals or barrier semaphores. Data moves between devices by JAX's collectives and lax.ppermute only.
A program may use at most 64 MiB of HBM per device.

```python
import jax
import jax.numpy as jnp
from jax import lax

D = 2048
FF = 2816
TOK_DEV = 160
TOKENS = 40960
N_REP = 64
N_FS = 4


def raised(values, own_key, source, target, shards_of, factor):
    def block_of(dim):
        return (jnp.arange(values.shape[dim]) // (values.shape[dim] // shards_of)).reshape((-1,) + (1,) * (values.ndim - 1 - dim))

    one_side = jax.random.permutation(own_key, shards_of)[block_of(target)]
    other_side = (block_of(target) + shards_of // 2) % shards_of
    return jnp.where((block_of(source) == one_side) | (block_of(source) == other_side), factor * values, values)


def levels(stream_key, extent, shards, least, high):
    level = 1.0
    for axis_at, shards_of in shards:
        steps = jax.random.uniform(jax.random.fold_in(jax.random.fold_in(stream_key, 6), axis_at), (shards_of,), jnp.float32, least / len(shards), high / len(shards))
        level = level * jnp.repeat(jnp.exp(steps), extent[axis_at] // shards_of).reshape((-1,) + (1,) * (len(extent) - 1 - axis_at))
    return level


def normal_values(rng, shape, spread, reach, pieces=(), held_as=jnp.bfloat16):
    array = jax.random.normal(rng, shape, jnp.float32) * spread
    if len(pieces) > 0:
        array = levels(rng, shape, pieces, -0.22, 0.18) * array
    return jnp.clip(array, min=-reach, max=reach).astype(held_as)


def gaussian_with(key, extent, scale, bound, pieces, heavy, kind=jnp.bfloat16):
    result = scale * jax.random.normal(key, extent, jnp.float32)
    if pieces:
        result = result * levels(key, extent, pieces, -0.22, 0.18)
    return jnp.clip(raised(result, jax.random.fold_in(key, 3), *heavy), -bound, bound).astype(kind)


def setup_inputs(seed: int = 0) -> dict:
    seeds = jax.random.split(jax.random.key(seed), 7)
    gate_pre = normal_values(seeds[0], (TOKENS, FF), 1.0, 6.0, ((0, 256), (1, 2)))
    up_pre = normal_values(seeds[1], (TOKENS, FF), 1.0, 6.0, ((0, 256), (1, 2)))
    gate_taps = normal_values(seeds[2], (3, FF), 0.6, 3.0, ((1, 2),))
    up_taps = normal_values(seeds[3], (3, FF), 0.6, 3.0, ((1, 2),))
    down_weight = normal_values(seeds[4], (FF, D), D ** -0.5, 0.125, ((0, 2), (1, 4)))
    cotangent = gaussian_with(seeds[5], (TOKENS, D), 1.0, 16.0, ((0, 64), (1, 4)), (0, 1, 64, 4.0))
    return {"gate_pre": gate_pre, "up_pre": up_pre, "gate_taps": gate_taps, "up_taps": up_taps, "down_weight": down_weight, "cotangent": cotangent}


def shift_conv(padded, tap_coef):
    return tap_coef[0] * padded[:, :-2] + tap_coef[1] * padded[:, 1:-1] + tap_coef[2] * padded[:, 2:]


def back_conv(padded, tap_coef):
    return tap_coef[2] * padded[:, :-2] + tap_coef[1] * padded[:, 1:-1] + tap_coef[0] * padded[:, 2:]


def reference(gate_pre, up_pre, gate_taps, up_taps, down_weight, cotangent):
    length = TOK_DEV * N_FS
    width = gate_pre.shape[1]
    gate_pad = jnp.pad(gate_pre.astype(jnp.float32).reshape(N_REP, length, width), ((0, 0), (2, 0), (0, 0)))
    up_pad = jnp.pad(up_pre.astype(jnp.float32).reshape(N_REP, length, width), ((0, 0), (2, 0), (0, 0)))
    gate_coef = gate_taps.astype(jnp.float32)
    up_coef = up_taps.astype(jnp.float32)
    gate_conv = shift_conv(gate_pad, gate_coef)
    up_conv = shift_conv(up_pad, up_coef)
    gate_sig = jax.nn.sigmoid(gate_conv)
    activated = gate_conv * gate_sig
    hidden = (activated * up_conv).astype(jnp.bfloat16).reshape(TOKENS, width)
    quarter = D // N_FS
    d_hidden = jnp.zeros((TOKENS, width), jnp.float32)
    for index in range(N_FS):
        part_sum = lax.dot_general(cotangent[:, index * quarter:(index + 1) * quarter],
                                   down_weight[:, index * quarter:(index + 1) * quarter],
                                   (((1,), (1,)), ((), ())), preferred_element_type=jnp.float32)
        rounded = lax.optimization_barrier(part_sum.astype(jnp.bfloat16))
        d_hidden = d_hidden + rounded.astype(jnp.float32)
    d_hidden = d_hidden.reshape(N_REP, length, width)
    d_gate = d_hidden * up_conv * gate_sig * (1.0 + gate_conv * (1.0 - gate_sig))
    d_up = d_hidden * activated
    gate_back = jnp.pad(d_gate, ((0, 0), (0, 2), (0, 0)))
    up_back = jnp.pad(d_up, ((0, 0), (0, 2), (0, 0)))
    grad_gate = back_conv(gate_back, gate_coef).astype(jnp.bfloat16).reshape(TOKENS, width)
    grad_up = back_conv(up_back, up_coef).astype(jnp.bfloat16).reshape(TOKENS, width)
    grad_scale = float(TOKENS) ** -0.5
    grad_gate_taps = jnp.stack([jnp.sum(d_gate * gate_pad[:, offset:offset + length], axis=(0, 1)) for offset in range(3)]) * grad_scale
    grad_up_taps = jnp.stack([jnp.sum(d_up * up_pad[:, offset:offset + length], axis=(0, 1)) for offset in range(3)]) * grad_scale
    grad_full = lax.dot_general(cotangent, hidden, (((0,), (0,)), ((), ())), preferred_element_type=jnp.float32) * grad_scale
    down_norms = jnp.sum(grad_full * grad_full, axis=0) / D
    grad_down = grad_full.reshape(N_FS, quarter, width)
    return grad_gate, grad_up, grad_gate_taps, grad_up_taps, grad_down, down_norms
```

```python
import jax
import jax.numpy as jnp
from jax import lax
from jax.sharding import Mesh
from jax.sharding import PartitionSpec as P

D = 2048
ZY = ("zh", "zl", "yh", "yl")
TOK = ("zh", "zl", "yh", "yl", "fs")
NEAR = ("zl", "yl", "fs")
FAR = ("zh", "yh")
HALO = 2
PAD = 8


def shifted(array, axis, by):
    count = lax.axis_size(axis)
    return lax.ppermute(array, axis, [(i, (i + by) % count) for i in range(count)])


def passed_along(array, axis, by):
    count = lax.axis_size(axis)
    pairs = [(i, i + by) for i in range(count) if 0 <= i + by < count]
    return lax.ppermute(array, axis, pairs)


def swap(array, axes):
    return lax.all_to_all(array, axes, 0, 0, tiled=True)


def total_over(array, axes):
    count = lax.axis_size(axes)
    sent = jnp.broadcast_to(array.astype(jnp.bfloat16)[None], (count, *array.shape))
    return lax.optimization_barrier(jnp.sum(swap(sent, axes).astype(jnp.float32), axis=0))


def shift_conv(padded, coef):
    return coef[0] * padded[:-2] + coef[1] * padded[1:-1] + coef[2] * padded[2:]


def back_conv(padded, coef):
    return coef[2] * padded[:-2] + coef[1] * padded[1:-1] + coef[0] * padded[2:]


def local(gate_pre, up_pre, gate_taps, up_taps, down_weight, cotangent):
    rows, width = gate_pre.shape
    n_fs = lax.axis_size("fs")
    me = lax.axis_index("fs")
    before = passed_along(jnp.stack([gate_pre[-HALO:], up_pre[-HALO:]]), "fs", 1)
    after = passed_along(jnp.stack([gate_pre[:HALO], up_pre[:HALO]]), "fs", -1)
    gate_pad = jnp.concatenate([before[0], gate_pre, after[0]], 0).astype(jnp.float32)
    up_pad = jnp.concatenate([before[1], up_pre, after[1]], 0).astype(jnp.float32)
    gate_coef = gate_taps.astype(jnp.float32)
    up_coef = up_taps.astype(jnp.float32)
    gate_conv = shift_conv(gate_pad, gate_coef)
    up_conv = shift_conv(up_pad, up_coef)
    gate_sig = jax.nn.sigmoid(gate_conv)
    activated = gate_conv * gate_sig
    hidden = (activated * up_conv)[:rows].astype(jnp.bfloat16)

    cot_pad = jnp.concatenate([cotangent, jnp.zeros((PAD, cotangent.shape[1]), jnp.bfloat16)], 0)

    def term_for(step):
        start = ((me + step) % n_fs) * rows
        block = lax.dynamic_slice_in_dim(cot_pad, start, rows + PAD, 0)
        return lax.dot_general(
            block, down_weight, (((1,), (1,)), ((), ())), preferred_element_type=jnp.float32
        ).astype(jnp.bfloat16)

    everyone = swap(jnp.broadcast_to(hidden[None], (n_fs, rows, width)), "fs")
    everyone, *terms = lax.optimization_barrier((everyone, *(term_for(k) for k in (0, 1, 3, 2))))
    terms[1:] = [shifted(term, "fs", step) for term, step in zip(terms[1:], (1, 3, 2))]
    partial = lax.dot_general(
        cotangent,
        everyone.reshape(n_fs * rows, width),
        (((0,), (0,)), ((), ())),
        preferred_element_type=jnp.float32,
    ).astype(jnp.bfloat16)
    n_rep = lax.axis_size(ZY)
    parts = swap(partial.reshape(n_rep, -1, width), ZY)
    parts, gate_conv, up_conv = lax.optimization_barrier((parts, gate_conv, up_conv))
    gate_sig = jax.nn.sigmoid(gate_conv)
    activated = gate_conv * gate_sig
    grad_scale = float(rows * n_rep * n_fs) ** (-0.5)
    grad_share = jnp.sum(parts.astype(jnp.float32), axis=0) * grad_scale
    norm_part = jnp.sum(grad_share * grad_share, axis=0)

    d_hidden = sum(term.astype(jnp.float32) for term in terms)[: rows + HALO]
    d_gate = d_hidden * up_conv * gate_sig * (1.0 + gate_conv * (1.0 - gate_sig))
    d_up = d_hidden * activated
    grad_gate = back_conv(d_gate, gate_coef).astype(jnp.bfloat16)
    grad_up = back_conv(d_up, up_coef).astype(jnp.bfloat16)
    small = jnp.stack(
        [jnp.sum(d_gate[:rows] * gate_pad[k : k + rows], axis=0) for k in range(3)]
        + [jnp.sum(d_up[:rows] * up_pad[k : k + rows], axis=0) for k in range(3)]
        + [norm_part, jnp.zeros_like(norm_part)]
    )
    small = total_over(total_over(small, NEAR), FAR)
    return (
        grad_gate,
        grad_up,
        small[:3] * grad_scale,
        small[3:6] * grad_scale,
        grad_share[None],
        small[6] / D,
    )


def solution(mesh):
    finer = Mesh(
        mesh.devices.reshape(4, 2, 4, 2, mesh.shape["fs"], mesh.shape["tp"]),
        ("zh", "zl", "yh", "yl", "fs", "tp"),
    )
    in_specs = (P(TOK, "tp"), P(TOK, "tp"), P(None, "tp"), P(None, "tp"), P("tp", "fs"), P(ZY, "fs"))
    out_specs = (P(TOK, "tp"), P(TOK, "tp"), P(None, "tp"), P(None, "tp"), P("fs", ZY, "tp"), P("tp"))
    return jax.shard_map(local, mesh=finer, in_specs=in_specs, out_specs=out_specs, check_vma=False)
```

```python
import functools

import jax
import jax.numpy as jnp
from jax import lax
from jax.experimental import pallas as pl
from jax.experimental.pallas import tpu as pltpu
from jax.sharding import Mesh
from jax.sharding import PartitionSpec as P


D = 2048
ZY = ("zh", "zl", "yh", "yl")
TOK = ("zh", "zl", "yh", "yl", "fs")
NEAR = ("zl", "yl", "fs")
FAR = ("zh", "yh")
HALO = 2
PAD = 8
LANE = 128
GROUP = 4
F32 = jnp.float32
BF16 = jnp.bfloat16


def passed_along(array, axis, by):
    count = lax.axis_size(axis)
    pairs = [(i, i + by) for i in range(count) if 0 <= i + by < count]
    return lax.ppermute(array, axis, pairs)


def swap(array, axes):
    return lax.all_to_all(array, axes, 0, 0, tiled=True)


def call(body, out_shape, flops=0, limit=8, **kw):
    return pl.pallas_call(
        body,
        out_shape=out_shape,
        compiler_params=pltpu.CompilerParams(vmem_limit_bytes=limit << 20),
        cost_estimate=pl.CostEstimate(flops=flops, bytes_accessed=1 << 20, transcendentals=0),
        **kw,
    )


def hidden_body(rows, width, gate_ref, up_ref, before_ref, gate_taps, up_taps, out_ref, held_ref):
    step = pl.program_id(0)
    block = gate_ref.shape[1]

    def conv(which, source, taps):
        held_ref[PAD - HALO : PAD] = before_ref[which].astype(F32)
        held_ref[PAD : PAD + rows] = source[...].astype(F32)
        total = taps[2:3].astype(F32) * held_ref[PAD : PAD + rows]
        for k in range(2):
            start = PAD - HALO + k
            total += taps[k : k + 1].astype(F32) * held_ref[start : start + rows]
        return total

    gate = conv(0, gate_ref, gate_taps)
    up = conv(1, up_ref, up_taps)
    value = gate * (1.0 / (1.0 + jnp.exp(-gate))) * up
    lane = lax.broadcasted_iota(jnp.int32, value.shape, 1) + step * block
    value = jnp.where(lane < width, value, 0.0).astype(BF16)
    for k in range(out_ref.shape[1]):
        out_ref[0, k] = value


def hidden_of(gate_pre, up_pre, before, gate_taps, up_taps, block, n_fs):
    rows, width = gate_pre.shape
    wide = pl.BlockSpec((rows, block), lambda i: (0, i))
    taps = pl.BlockSpec((3, block), lambda i: (0, i))
    return call(
        functools.partial(hidden_body, rows, width),
        jax.ShapeDtypeStruct((GROUP, n_fs, rows, block), BF16),
        flops=40 * rows * width,
        limit=60,
        grid=(GROUP,),
        in_specs=[wide, wide, pl.BlockSpec((2, HALO, block), lambda i: (0, 0, i)), taps, taps],
        out_specs=pl.BlockSpec((1, n_fs, rows, block), lambda i: (i, 0, 0, 0)),
        scratch_shapes=[pltpu.VMEM((rows + PAD, block), F32)],
    )(gate_pre, up_pre, before, gate_taps, up_taps)


def terms_body(rows, at_ref, cot_ref, weight_ref, *refs):
    *outs, held_ref = refs
    tokens = cot_ref.shape[0]
    held_ref[:tokens] = cot_ref[...]
    held_ref[tokens:] = jnp.zeros((held_ref.shape[0] - tokens, held_ref.shape[1]), BF16)
    for k, out in enumerate(outs):
        start = pl.multiple_of(at_ref[k] * rows, 16)
        out[...] = lax.dot_general(
            held_ref[pl.ds(start, rows + PAD)],
            weight_ref[...],
            (((1,), (1,)), ((), ())),
            preferred_element_type=F32,
        ).astype(BF16)


def terms_of(at, cotangent, weight, rows):
    tokens, depth = cotangent.shape
    width = weight.shape[0]
    whole = pl.BlockSpec(memory_space=pltpu.VMEM)
    steps = tokens // rows
    return call(
        functools.partial(terms_body, rows),
        (jax.ShapeDtypeStruct((rows + PAD, width), BF16),) * steps,
        flops=2 * tokens * depth * width,
        limit=16,
        in_specs=[pl.BlockSpec(memory_space=pltpu.SMEM), whole, whole],
        out_specs=(whole,) * steps,
        scratch_shapes=[pltpu.VMEM((tokens + 2 * PAD, depth), BF16)],
    )(at, cotangent, weight)


def grad_body(order_ref, own_ref, side_ref, far_ref, across_ref, hidden_ref, out_ref, total_ref):
    step = pl.program_id(0)
    for k, ref in enumerate((own_ref, side_ref, far_ref)):

        @pl.when(step == k)
        def _(ref=ref, k=k):
            part = lax.dot_general(
                ref[...], hidden_ref[0], (((0,), (0,)), ((), ())), preferred_element_type=F32
            )
            total_ref[...] = part if k == 0 else total_ref[...] + part

    @pl.when(step >= 3)
    def _():
        part = lax.dot_general(
            across_ref[0], hidden_ref[0], (((0,), (0,)), ((), ())), preferred_element_type=F32
        )
        total_ref[...] += part

    @pl.when(step == pl.num_programs(0) - 1)
    def _():
        out_ref[...] = total_ref[...].astype(BF16).reshape(out_ref.shape)


def grad_of(order, own, side, far, across, hidden, n_rep):
    tokens, depth = own.shape
    block = hidden.shape[2]
    shape = (n_rep, depth // n_rep, block)
    same = pl.BlockSpec((tokens, depth), lambda i, order: (0, 0))
    return call(
        grad_body,
        jax.ShapeDtypeStruct(shape, BF16),
        flops=2 * GROUP * tokens * depth * block,
        limit=60,
        grid_spec=pltpu.PrefetchScalarGridSpec(
            num_scalar_prefetch=1,
            grid=(GROUP + 1,),
            in_specs=[same] * 3
            + [
                pl.BlockSpec(
                    (1, tokens, depth), lambda i, order: (jnp.maximum(i - 3, 0), 0, 0)
                ),
                pl.BlockSpec((1, tokens, block), lambda i, order: (order[i], 0, 0)),
            ],
            out_specs=pl.BlockSpec(shape, lambda i, order: (0, 0, 0)),
            scratch_shapes=[pltpu.VMEM((depth, block), F32)],
        ),
    )(order, own, side, far, across, hidden)


def share_body(scale, parts_ref, taps_ref, grad_ref, small_ref):
    block = parts_ref.shape[2]
    copies, rows, width = small_ref.shape
    for zl in range(2):
        for yl in range(2):
            total = None
            for zh in range(4):
                for yh in range(4):
                    part = parts_ref[((zh * 2 + zl) * 4 + yh) * 2 + yl].astype(F32)
                    total = part if total is None else total + part
            start = (zl * 2 + yl) * block
            size = min(block, width - start)
            grad_ref[:, start : start + size] = total[:, :size] * scale
    value = grad_ref[...]
    norm = jnp.sum(value * value, axis=0, keepdims=True)
    row = lax.broadcasted_iota(jnp.int32, (rows, width), 0)
    small = jnp.where(row == rows - 1, norm, taps_ref[...]).astype(BF16)
    for k in range(copies):
        small_ref[k] = small


def chain_body(rows, *refs):
    *terms, gate_ref, up_ref, before_ref, after_ref, gate_taps, up_taps = refs[:10]
    gate_out, up_out, taps_out, gate_held, up_held, gate_back, up_back = refs[10:]
    reach = terms[0].shape[0]
    for at in range(0, gate_ref.shape[1], LANE):
        lanes = slice(at, at + LANE)

        def conv(which, source, taps, held):
            held[PAD - HALO : PAD] = before_ref[which, :, lanes].astype(F32)
            held[PAD : PAD + rows] = source[:, lanes].astype(F32)
            held[PAD + rows : PAD + rows + HALO] = after_ref[which, :, lanes].astype(F32)
            coef = [taps[k : k + 1, lanes].astype(F32) for k in range(3)]
            total = coef[2] * held[PAD : PAD + reach]
            for k in range(2):
                total += coef[k] * held[PAD - HALO + k : PAD - HALO + k + reach]
            return total, coef

        gate, gate_coef = conv(0, gate_ref, gate_taps, gate_held)
        up, up_coef = conv(1, up_ref, up_taps, up_held)
        d_hidden = terms[0][:, lanes].astype(F32)
        for term in terms[1:]:
            d_hidden += term[:, lanes].astype(F32)
        sig = 1.0 / (1.0 + jnp.exp(-gate))
        gate_back[...] = d_hidden * up * sig * (1.0 + gate * (1.0 - sig))
        up_back[...] = d_hidden * gate * sig

        def back(coef, held, out):
            total = coef[2] * held[:rows]
            for k in range(2):
                total += coef[k] * held[2 - k : 2 - k + rows]
            out[:, lanes] = total.astype(BF16)

        back(gate_coef, gate_back, gate_out)
        back(up_coef, up_back, up_out)
        for first, held, source in ((0, gate_back, gate_held), (3, up_back, up_held)):
            for k in range(3):
                start = PAD - HALO + k
                product = held[:rows] * source[start : start + rows]
                taps_out[first + k : first + k + 1, lanes] = jnp.sum(product, 0, keepdims=True)
        taps_out[6:, lanes] = jnp.zeros((2, LANE), F32)


def chain_of(terms, gate_pre, up_pre, before, after, gate_taps, up_taps, block):
    rows, width = gate_pre.shape
    reach = terms[0].shape[0]
    tall = pl.BlockSpec((reach, block), lambda i: (0, i))
    wide = pl.BlockSpec((rows, block), lambda i: (0, i))
    edge = pl.BlockSpec((2, HALO, block), lambda i: (0, 0, i))
    taps = pl.BlockSpec((3, block), lambda i: (0, i))
    grad = jax.ShapeDtypeStruct((rows, width), BF16)
    return call(
        functools.partial(chain_body, rows),
        (grad, grad, jax.ShapeDtypeStruct((8, width), F32)),
        flops=100 * rows * width,
        limit=60,
        grid=(GROUP,),
        in_specs=[tall] * 4 + [wide, wide, edge, edge, taps, taps],
        out_specs=(wide, wide, pl.BlockSpec((8, block), lambda i: (0, i))),
        scratch_shapes=[pltpu.VMEM((reach + PAD, LANE), F32)] * 2
        + [pltpu.VMEM((reach, LANE), F32)] * 2,
    )(*terms, gate_pre, up_pre, before, after, gate_taps, up_taps)


def total_of(seen_ref):
    total = None
    for source in range(seen_ref.shape[0]):
        part = seen_ref[source].astype(F32)
        total = part if total is None else total + part
    return total


def middle_body(seen_ref, small_ref):
    total = total_of(seen_ref).astype(BF16)
    for k in range(small_ref.shape[0]):
        small_ref[k] = total


def last_body(scale, seen_ref, gate_ref, up_ref, norm_ref):
    total = total_of(seen_ref)
    gate_ref[...] = total[:3] * scale
    up_ref[...] = total[3:6] * scale
    norm_ref[...] = total[7:] / D


def local(gate_pre, up_pre, gate_taps, up_taps, down_weight, cotangent):
    rows, width = gate_pre.shape
    n_fs = lax.axis_size("fs")
    n_rep = lax.axis_size(ZY)
    n_near = lax.axis_size(NEAR)
    n_far = lax.axis_size(FAR)
    block = -(-(width // LANE) // GROUP) * LANE
    grad_scale = float(rows * n_rep * n_fs) ** (-0.5)

    before = passed_along(jnp.stack([gate_pre[-HALO:], up_pre[-HALO:]]), "fs", 1)
    after = passed_along(jnp.stack([gate_pre[:HALO], up_pre[:HALO]]), "fs", -1)

    axes = ("zl", "yl", "tp")
    first, second = [], []
    for i in range(8):
        flip = 4 if i % 2 == 0 else 2
        first.append((i, i ^ flip))
        if i % 2 == 0:
            second.append((i, i ^ 6))
    side = lax.ppermute(cotangent, axes, first)
    far = lax.ppermute(cotangent, axes, second)
    across = lax.ppermute(jnp.stack([side, far]), "tp", [(0, 1), (1, 0)])
    tp = lax.axis_index("tp")
    member = lax.axis_index("zl") * 2 + lax.axis_index("yl")
    order = jnp.stack(
        [member, member ^ (2 - tp), member ^ 3, member ^ (1 + tp), member ^ 3]
    )

    hidden = hidden_of(gate_pre, up_pre, before, gate_taps, up_taps, block, n_fs)
    everyone = swap(hidden.reshape(n_near, rows, block), NEAR)

    me = lax.axis_index("fs")
    steps = (1, 3, 2, 0)
    hidden, cot_late = lax.optimization_barrier((hidden, cotangent))
    at = jnp.stack([(me + step) % n_fs for step in steps])
    terms = list(terms_of(at, cot_late, down_weight, rows))
    for k, step in enumerate(steps[:3]):
        pairs = [(i, (i + step) % n_fs) for i in range(n_fs)]
        terms[k] = lax.ppermute(terms[k], "fs", pairs)

    partial = grad_of(
        order, cotangent, side, far, across, everyone.reshape(GROUP, -1, block), n_rep
    )
    parts = swap(partial, ZY)

    grad_gate, grad_up, taps = chain_of(
        terms, gate_pre, up_pre, before, after, gate_taps, up_taps, block
    )

    wide = jax.ShapeDtypeStruct((8, width), F32)
    sent = functools.partial(jax.ShapeDtypeStruct, dtype=BF16)
    grad_share, small = call(
        functools.partial(share_body, grad_scale), (wide, sent((n_near, 8, width)))
    )(parts, taps)
    small = call(middle_body, sent((n_far, 8, width)))(swap(small, NEAR))
    three = jax.ShapeDtypeStruct((3, width), F32)
    gate_out, up_out, norms = call(
        functools.partial(last_body, grad_scale),
        (three, three, jax.ShapeDtypeStruct((1, width), F32)),
    )(swap(small, FAR))
    return grad_gate, grad_up, gate_out, up_out, grad_share[None], norms[0]


def solution(mesh):
    finer = Mesh(
        mesh.devices.reshape(4, 2, 4, 2, mesh.shape["fs"], mesh.shape["tp"]),
        ("zh", "zl", "yh", "yl", "fs", "tp"),
    )
    in_specs = (P(TOK, "tp"), P(TOK, "tp"), P(None, "tp"), P(None, "tp"), P("tp", "fs"), P(ZY, "fs"))
    out_specs = (P(TOK, "tp"), P(TOK, "tp"), P(None, "tp"), P(None, "tp"), P("fs", ZY, "tp"), P("tp"))
    return jax.shard_map(local, mesh=finer, in_specs=in_specs, out_specs=out_specs, check_vma=False)
```

```python
import functools

import jax
import jax.numpy as jnp
from jax import lax
from jax.experimental import pallas as pl
from jax.experimental.pallas import tpu as pltpu
from jax.sharding import Mesh
from jax.sharding import PartitionSpec as P


D = 2048
ZY = ("zh", "zl", "yh", "yl")
TOK = ("zh", "zl", "yh", "yl", "fs")
NEAR = ("zl", "yl", "fs")
FAR = ("zh", "yh")
HALO = 2
PAD = 8
LANE = 128
GROUP = 4
F32 = jnp.float32
BF16 = jnp.bfloat16


def passed_along(array, axis, by):
    count = lax.axis_size(axis)
    pairs = [(i, i + by) for i in range(count) if 0 <= i + by < count]
    return lax.ppermute(array, axis, pairs)


def swap(array, axes):
    return lax.all_to_all(array, axes, 0, 0, tiled=True)


def call(body, out_shape, flops=0, limit=8, **kw):
    return pl.pallas_call(
        body,
        out_shape=out_shape,
        compiler_params=pltpu.CompilerParams(vmem_limit_bytes=limit << 20),
        cost_estimate=pl.CostEstimate(flops=flops, bytes_accessed=1 << 20, transcendentals=0),
        **kw,
    )


def hidden_body(rows, width, gate_ref, up_ref, before_ref, gate_taps, up_taps, out_ref, held_ref):
    step = pl.program_id(0)
    block = gate_ref.shape[1]

    def conv(which, source, taps):
        held_ref[PAD - HALO : PAD] = before_ref[which].astype(F32)
        held_ref[PAD : PAD + rows] = source[...].astype(F32)
        total = taps[2:3].astype(F32) * held_ref[PAD : PAD + rows]
        for k in range(2):
            start = PAD - HALO + k
            total += taps[k : k + 1].astype(F32) * held_ref[start : start + rows]
        return total

    gate = conv(0, gate_ref, gate_taps)
    up = conv(1, up_ref, up_taps)
    value = gate * (1.0 / (1.0 + jnp.exp(-gate))) * up
    lane = lax.broadcasted_iota(jnp.int32, value.shape, 1) + step * block
    value = jnp.where(lane < width, value, 0.0).astype(BF16)
    for k in range(out_ref.shape[1]):
        out_ref[0, k] = value


def hidden_of(gate_pre, up_pre, before, gate_taps, up_taps, block, n_fs):
    rows, width = gate_pre.shape
    wide = pl.BlockSpec((rows, block), lambda i: (0, i))
    taps = pl.BlockSpec((3, block), lambda i: (0, i))
    return call(
        functools.partial(hidden_body, rows, width),
        jax.ShapeDtypeStruct((GROUP, n_fs, rows, block), BF16),
        flops=40 * rows * width,
        limit=60,
        grid=(GROUP,),
        in_specs=[wide, wide, pl.BlockSpec((2, HALO, block), lambda i: (0, 0, i)), taps, taps],
        out_specs=pl.BlockSpec((1, n_fs, rows, block), lambda i: (i, 0, 0, 0)),
        scratch_shapes=[pltpu.VMEM((rows + PAD, block), F32)],
    )(gate_pre, up_pre, before, gate_taps, up_taps)


def terms_body(rows, at_ref, cot_ref, weight_ref, *refs):
    *outs, held_ref = refs
    tokens = cot_ref.shape[0]
    held_ref[:tokens] = cot_ref[...]
    held_ref[tokens:] = jnp.zeros((held_ref.shape[0] - tokens, held_ref.shape[1]), BF16)
    for k, out in enumerate(outs):
        start = pl.multiple_of(at_ref[k] * rows, 16)
        out[...] = lax.dot_general(
            held_ref[pl.ds(start, rows + PAD)],
            weight_ref[...],
            (((1,), (1,)), ((), ())),
            preferred_element_type=F32,
        ).astype(BF16)


def terms_of(at, cotangent, weight, rows):
    tokens, depth = cotangent.shape
    width = weight.shape[0]
    whole = pl.BlockSpec(memory_space=pltpu.VMEM)
    steps = tokens // rows
    return call(
        functools.partial(terms_body, rows),
        (jax.ShapeDtypeStruct((rows + PAD, width), BF16),) * steps,
        flops=2 * tokens * depth * width,
        limit=16,
        in_specs=[pl.BlockSpec(memory_space=pltpu.SMEM), whole, whole],
        out_specs=(whole,) * steps,
        scratch_shapes=[pltpu.VMEM((tokens + 2 * PAD, depth), BF16)],
    )(at, cotangent, weight)


def grad_body(order_ref, own, side, far, across, hidden, out_ref, cot_ref, rows_ref, cot_sem, row_sem):
    tokens = own.shape[0]
    core = order_ref[GROUP]

    def fetch(k, source):
        spot = pl.ds(k * tokens, tokens)
        return pltpu.make_async_copy(source, cot_ref.at[spot], cot_sem.at[k])

    def fetch_rows(k):
        spot = pl.ds(k * tokens, tokens)
        return pltpu.make_async_copy(hidden.at[order_ref[k]], rows_ref.at[spot], row_sem.at[k])

    blocks = [fetch(0, own), fetch(1, side), fetch(2, across.at[0])]
    for k, copy in enumerate(blocks):
        copy.start()
        fetch_rows(k).start()

    @pl.when(core == 0)
    def _():
        fetch(3, far).start()

    @pl.when(core != 0)
    def _():
        fetch(3, across.at[1]).start()

    fetch_rows(3).start()
    total = None
    for part in range(2):
        for k in (2 * part, 2 * part + 1):
            fetch(k, own).wait()
            fetch_rows(k).wait()
        span = slice(2 * part * tokens, 2 * (part + 1) * tokens)
        value = lax.dot_general(
            cot_ref[span], rows_ref[span], (((0,), (0,)), ((), ())), preferred_element_type=F32
        )
        total = value if total is None else total + value
    out_ref[...] = total.astype(BF16).reshape(out_ref.shape)


def grad_of(order, own, side, far, across, hidden, n_rep):
    tokens, depth = own.shape
    block = hidden.shape[2]
    return call(
        grad_body,
        jax.ShapeDtypeStruct((n_rep, depth // n_rep, block), BF16),
        flops=2 * GROUP * tokens * depth * block,
        limit=60,
        in_specs=[pl.BlockSpec(memory_space=pltpu.SMEM)] + [pl.BlockSpec(memory_space=pl.ANY)] * 5,
        out_specs=pl.BlockSpec(memory_space=pltpu.VMEM),
        scratch_shapes=[
            pltpu.VMEM((GROUP * tokens, depth), BF16),
            pltpu.VMEM((GROUP * tokens, block), BF16),
            pltpu.SemaphoreType.DMA((GROUP,)),
            pltpu.SemaphoreType.DMA((GROUP,)),
        ],
    )(order, own, side, far, across, hidden)


def share_body(scale, parts_ref, taps_ref, grad_ref, small_ref):
    block = parts_ref.shape[2]
    rows, width = taps_ref.shape
    copies = small_ref.shape[0] // GROUP
    for zl in range(2):
        for yl in range(2):
            total = None
            for zh in range(4):
                for yh in range(4):
                    part = parts_ref[((zh * 2 + zl) * 4 + yh) * 2 + yl].astype(F32)
                    total = part if total is None else total + part
            start = (zl * 2 + yl) * block
            size = min(block, width - start)
            grad_ref[:, start : start + size] = total[:, :size] * scale
    value = grad_ref[...]
    norm = jnp.sum(value * value, axis=0, keepdims=True)
    row = lax.broadcasted_iota(jnp.int32, (rows, width), 0)
    small = jnp.where(row == rows - 1, norm, taps_ref[...]).astype(BF16)
    for member in range(GROUP):
        start = member * block
        size = min(block, width - start)
        for k in range(member * copies, (member + 1) * copies):
            small_ref[k, :, :size] = small[:, start : start + size]
            if size < block:
                small_ref[k, :, size:] = jnp.zeros((rows, block - size), BF16)


def chain_body(rows, *refs):
    *terms, gate_ref, up_ref, before_ref, after_ref, gate_taps, up_taps = refs[:10]
    gate_out, up_out, taps_out, gate_held, up_held, gate_back, up_back = refs[10:]
    reach = terms[0].shape[0]
    for at in range(0, gate_ref.shape[1], LANE):
        lanes = slice(at, at + LANE)

        def conv(which, source, taps, held):
            held[PAD - HALO : PAD] = before_ref[which, :, lanes].astype(F32)
            held[PAD : PAD + rows] = source[:, lanes].astype(F32)
            held[PAD + rows : PAD + rows + HALO] = after_ref[which, :, lanes].astype(F32)
            coef = [taps[k : k + 1, lanes].astype(F32) for k in range(3)]
            total = coef[2] * held[PAD : PAD + reach]
            for k in range(2):
                total += coef[k] * held[PAD - HALO + k : PAD - HALO + k + reach]
            return total, coef

        gate, gate_coef = conv(0, gate_ref, gate_taps, gate_held)
        up, up_coef = conv(1, up_ref, up_taps, up_held)
        d_hidden = terms[0][:, lanes].astype(F32)
        for term in terms[1:]:
            d_hidden += term[:, lanes].astype(F32)
        sig = 1.0 / (1.0 + jnp.exp(-gate))
        gate_back[...] = d_hidden * up * sig * (1.0 + gate * (1.0 - sig))
        up_back[...] = d_hidden * gate * sig

        def back(coef, held, out):
            total = coef[2] * held[:rows]
            for k in range(2):
                total += coef[k] * held[2 - k : 2 - k + rows]
            out[:, lanes] = total.astype(BF16)

        back(gate_coef, gate_back, gate_out)
        back(up_coef, up_back, up_out)
        for first, held, source in ((0, gate_back, gate_held), (3, up_back, up_held)):
            for k in range(3):
                start = PAD - HALO + k
                product = held[:rows] * source[start : start + rows]
                taps_out[first + k : first + k + 1, lanes] = jnp.sum(product, 0, keepdims=True)
        taps_out[6:, lanes] = jnp.zeros((2, LANE), F32)


def chain_of(terms, gate_pre, up_pre, before, after, gate_taps, up_taps, block):
    rows, width = gate_pre.shape
    reach = terms[0].shape[0]
    tall = pl.BlockSpec((reach, block), lambda i: (0, i))
    wide = pl.BlockSpec((rows, block), lambda i: (0, i))
    edge = pl.BlockSpec((2, HALO, block), lambda i: (0, 0, i))
    taps = pl.BlockSpec((3, block), lambda i: (0, i))
    grad = jax.ShapeDtypeStruct((rows, width), BF16)
    return call(
        functools.partial(chain_body, rows),
        (grad, grad, jax.ShapeDtypeStruct((8, width), F32)),
        flops=100 * rows * width,
        limit=60,
        grid=(GROUP,),
        in_specs=[tall] * 4 + [wide, wide, edge, edge, taps, taps],
        out_specs=(wide, wide, pl.BlockSpec((8, block), lambda i: (0, i))),
        scratch_shapes=[pltpu.VMEM((reach + PAD, LANE), F32)] * 2
        + [pltpu.VMEM((reach, LANE), F32)] * 2,
    )(*terms, gate_pre, up_pre, before, after, gate_taps, up_taps)


def total_of(seen_ref):
    total = None
    for source in range(seen_ref.shape[0]):
        part = seen_ref[source].astype(F32)
        total = part if total is None else total + part
    return total


def middle_body(seen_ref, small_ref):
    total = total_of(seen_ref).astype(small_ref.dtype)
    for k in range(small_ref.shape[0]):
        small_ref[k] = total


def last_body(scale, seen_ref, gate_ref, up_ref, norm_ref):
    block = seen_ref.shape[2]
    for member in range(GROUP):
        start = member * block
        size = min(block, gate_ref.shape[1] - start)
        lanes = slice(start, start + size)
        gate_ref[:, lanes] = seen_ref[member, :3, :size] * scale
        up_ref[:, lanes] = seen_ref[member, 3:6, :size] * scale
        norm_ref[:, lanes] = seen_ref[member, 7:, :size] / D


def local(gate_pre, up_pre, gate_taps, up_taps, down_weight, cotangent):
    rows, width = gate_pre.shape
    n_fs = lax.axis_size("fs")
    n_rep = lax.axis_size(ZY)
    n_near = lax.axis_size(NEAR)
    n_far = lax.axis_size(FAR)
    block = -(-(width // LANE) // GROUP) * LANE
    grad_scale = float(rows * n_rep * n_fs) ** (-0.5)

    before = passed_along(jnp.stack([gate_pre[-HALO:], up_pre[-HALO:]]), "fs", 1)
    after = passed_along(jnp.stack([gate_pre[:HALO], up_pre[:HALO]]), "fs", -1)

    axes = ("zl", "yl", "tp")
    first, second = [], []
    for i in range(8):
        flip = 4 if i % 2 == 0 else 2
        first.append((i, i ^ flip))
        if i % 2 == 0:
            second.append((i, i ^ 6))
    side = lax.ppermute(cotangent, axes, first)
    far = lax.ppermute(cotangent, axes, second)
    across = lax.ppermute(jnp.stack([side, far]), "tp", [(0, 1), (1, 0)])
    tp = lax.axis_index("tp")
    member = lax.axis_index("zl") * 2 + lax.axis_index("yl")
    order = jnp.stack(
        [member, member ^ (2 - tp), member ^ (1 + tp), member ^ 3, tp]
    )

    hidden = hidden_of(gate_pre, up_pre, before, gate_taps, up_taps, block, n_fs)
    everyone = swap(hidden.reshape(n_near, rows, block), NEAR)

    me = lax.axis_index("fs")
    steps = (1, 3, 2, 0)
    hidden, cot_late = lax.optimization_barrier((hidden, cotangent))
    at = jnp.stack([(me + step) % n_fs for step in steps])
    terms = list(terms_of(at, cot_late, down_weight, rows))
    for k, step in enumerate(steps[:3]):
        pairs = [(i, (i + step) % n_fs) for i in range(n_fs)]
        terms[k] = lax.ppermute(terms[k], "fs", pairs)

    partial = grad_of(
        order, cotangent, side, far, across, everyone.reshape(GROUP, -1, block), n_rep
    )
    parts = swap(partial, ZY)

    grad_gate, grad_up, taps = chain_of(
        terms, gate_pre, up_pre, before, after, gate_taps, up_taps, block
    )

    sent = jax.ShapeDtypeStruct((n_near, 8, block), BF16)
    grad_share, small = call(
        functools.partial(share_body, grad_scale), (jax.ShapeDtypeStruct((8, width), F32), sent)
    )(parts, taps)
    small = call(middle_body, jax.ShapeDtypeStruct((n_far, 8, block), BF16))(swap(small, NEAR))
    small = call(middle_body, jax.ShapeDtypeStruct((GROUP, 8, block), F32))(swap(small, FAR))
    three = jax.ShapeDtypeStruct((3, width), F32)
    gate_out, up_out, norms = call(
        functools.partial(last_body, grad_scale),
        (three, three, jax.ShapeDtypeStruct((1, width), F32)),
    )(swap(small, ("zl", "yl")))
    return grad_gate, grad_up, gate_out, up_out, grad_share[None], norms[0]


def solution(mesh):
    finer = Mesh(
        mesh.devices.reshape(4, 2, 4, 2, mesh.shape["fs"], mesh.shape["tp"]),
        ("zh", "zl", "yh", "yl", "fs", "tp"),
    )
    in_specs = (P(TOK, "tp"), P(TOK, "tp"), P(None, "tp"), P(None, "tp"), P("tp", "fs"), P(ZY, "fs"))
    out_specs = (P(TOK, "tp"), P(TOK, "tp"), P(None, "tp"), P(None, "tp"), P("fs", ZY, "tp"), P("tp"))
    return jax.shard_map(local, mesh=finer, in_specs=in_specs, out_specs=out_specs, check_vma=False)
```

```python
import functools

import jax
import jax.numpy as jnp
from jax import lax
from jax.experimental import pallas as pl
from jax.experimental.pallas import tpu as pltpu
from jax.sharding import Mesh
from jax.sharding import PartitionSpec as P


D = 2048
ZY = ("zh", "zl", "yh", "yl")
TOK = ("zh", "zl", "yh", "yl", "fs")
NEAR = ("zl", "yl", "fs")
FAR = ("zh", "yh")
HALO = 2
PAD = 8
LANE = 128
GROUP = 4
F32 = jnp.float32
BF16 = jnp.bfloat16


def passed_along(array, axis, by):
    count = lax.axis_size(axis)
    pairs = [(i, i + by) for i in range(count) if 0 <= i + by < count]
    return lax.ppermute(array, axis, pairs)


def swap(array, axes):
    return lax.all_to_all(array, axes, 0, 0, tiled=True)


def call(body, out_shape, flops=0, limit=8, **kw):
    return pl.pallas_call(
        body,
        out_shape=out_shape,
        compiler_params=pltpu.CompilerParams(vmem_limit_bytes=limit << 20),
        cost_estimate=pl.CostEstimate(flops=flops, bytes_accessed=1 << 20, transcendentals=0),
        **kw,
    )


def hidden_body(rows, width, gate_ref, up_ref, before_ref, gate_taps, up_taps, out_ref, held_ref):
    step = pl.program_id(0)
    block = gate_ref.shape[1]

    def conv(which, source, taps):
        held_ref[PAD - HALO : PAD] = before_ref[which].astype(F32)
        held_ref[PAD : PAD + rows] = source[...].astype(F32)
        total = taps[2:3].astype(F32) * held_ref[PAD : PAD + rows]
        for k in range(2):
            start = PAD - HALO + k
            total += taps[k : k + 1].astype(F32) * held_ref[start : start + rows]
        return total

    gate = conv(0, gate_ref, gate_taps)
    up = conv(1, up_ref, up_taps)
    value = gate * (1.0 / (1.0 + jnp.exp(-gate))) * up
    lane = lax.broadcasted_iota(jnp.int32, value.shape, 1) + step * block
    value = jnp.where(lane < width, value, 0.0).astype(BF16)
    for k in range(out_ref.shape[1]):
        out_ref[0, k] = value


def hidden_of(gate_pre, up_pre, before, gate_taps, up_taps, block, n_fs):
    rows, width = gate_pre.shape
    wide = pl.BlockSpec((rows, block), lambda i: (0, i))
    taps = pl.BlockSpec((3, block), lambda i: (0, i))
    return call(
        functools.partial(hidden_body, rows, width),
        jax.ShapeDtypeStruct((GROUP, n_fs, rows, block), BF16),
        flops=40 * rows * width,
        limit=60,
        grid=(GROUP,),
        in_specs=[wide, wide, pl.BlockSpec((2, HALO, block), lambda i: (0, 0, i)), taps, taps],
        out_specs=pl.BlockSpec((1, n_fs, rows, block), lambda i: (i, 0, 0, 0)),
        scratch_shapes=[pltpu.VMEM((rows + PAD, block), F32)],
    )(gate_pre, up_pre, before, gate_taps, up_taps)


def terms_body(rows, at_ref, cot_ref, weight_ref, *refs):
    *outs, held_ref = refs
    tokens = cot_ref.shape[0]
    held_ref[:tokens] = cot_ref[...]
    held_ref[tokens:] = jnp.zeros((held_ref.shape[0] - tokens, held_ref.shape[1]), BF16)
    for k, out in enumerate(outs):
        start = pl.multiple_of(at_ref[k] * rows, 16)
        out[...] = lax.dot_general(
            held_ref[pl.ds(start, rows + PAD)],
            weight_ref[...],
            (((1,), (1,)), ((), ())),
            preferred_element_type=F32,
        ).astype(BF16)


def terms_of(at, cotangent, weight, rows):
    tokens, depth = cotangent.shape
    width = weight.shape[0]
    whole = pl.BlockSpec(memory_space=pltpu.VMEM)
    steps = tokens // rows
    return call(
        functools.partial(terms_body, rows),
        (jax.ShapeDtypeStruct((rows + PAD, width), BF16),) * steps,
        flops=2 * tokens * depth * width,
        limit=16,
        in_specs=[pl.BlockSpec(memory_space=pltpu.SMEM), whole, whole],
        out_specs=(whole,) * steps,
        scratch_shapes=[pltpu.VMEM((tokens + 2 * PAD, depth), BF16)],
    )(at, cotangent, weight)


def turn_body(core_ref, own_ref, side_ref, far_ref, across_ref, out_ref):
    step = pl.program_id(0)
    core = core_ref[0]
    cases = (
        (step == 0, lambda: own_ref[...]),
        (step == 1, lambda: side_ref[...]),
        (step == 2, lambda: across_ref[0]),
        ((step == 3) & (core == 0), lambda: far_ref[...]),
        ((step == 3) & (core != 0), lambda: across_ref[1]),
    )
    for case, block in cases:

        @pl.when(case)
        def _(block=block):
            out_ref[...] = block().T


def turn_of(core, own, side, far, across):
    tokens, depth = own.shape
    same = pl.BlockSpec((tokens, depth), lambda i: (0, 0))
    return call(
        turn_body,
        jax.ShapeDtypeStruct((depth, GROUP * tokens), BF16),
        flops=tokens * depth,
        limit=60,
        grid=(GROUP,),
        in_specs=[pl.BlockSpec(memory_space=pltpu.SMEM)]
        + [same] * 3
        + [pl.BlockSpec((2, tokens, depth), lambda i: (0, 0, 0))],
        out_specs=pl.BlockSpec((depth, tokens), lambda i: (0, i)),
    )(core, own, side, far, across)


def grad_body(order_ref, turned, hidden, out_ref, cot_ref, rows_ref, cot_sem, row_sem):
    tokens = hidden.shape[1]

    def fetch(part):
        spot = pl.ds(2 * part * tokens, 2 * tokens)
        return pltpu.make_async_copy(turned.at[:, spot], cot_ref.at[:, spot], cot_sem.at[part])

    def fetch_rows(k):
        spot = pl.ds(k * tokens, tokens)
        return pltpu.make_async_copy(hidden.at[order_ref[k]], rows_ref.at[spot], row_sem.at[k])

    for part in range(2):
        fetch(part).start()
        fetch_rows(2 * part).start()
        fetch_rows(2 * part + 1).start()
    total = None
    for part in range(2):
        fetch(part).wait()
        fetch_rows(2 * part).wait()
        fetch_rows(2 * part + 1).wait()
        span = slice(2 * part * tokens, 2 * (part + 1) * tokens)
        value = jnp.dot(cot_ref[:, span], rows_ref[span], preferred_element_type=F32)
        total = value if total is None else total + value
    out_ref[...] = total.astype(BF16).reshape(out_ref.shape)


def grad_of(order, turned, hidden, n_rep):
    depth, tokens = turned.shape
    block = hidden.shape[2]
    return call(
        grad_body,
        jax.ShapeDtypeStruct((n_rep, depth // n_rep, block), BF16),
        flops=2 * tokens * depth * block,
        limit=60,
        in_specs=[pl.BlockSpec(memory_space=pltpu.SMEM)] + [pl.BlockSpec(memory_space=pl.ANY)] * 2,
        out_specs=pl.BlockSpec(memory_space=pltpu.VMEM),
        scratch_shapes=[
            pltpu.VMEM((depth, tokens), BF16),
            pltpu.VMEM((tokens, block), BF16),
            pltpu.SemaphoreType.DMA((2,)),
            pltpu.SemaphoreType.DMA((GROUP,)),
        ],
    )(order, turned, hidden)


def share_body(scale, parts_ref, taps_ref, grad_ref, small_ref):
    block = parts_ref.shape[2]
    rows, width = taps_ref.shape
    copies = small_ref.shape[0] // GROUP
    for zl in range(2):
        for yl in range(2):
            total = None
            for zh in range(4):
                for yh in range(4):
                    part = parts_ref[((zh * 2 + zl) * 4 + yh) * 2 + yl].astype(F32)
                    total = part if total is None else total + part
            start = (zl * 2 + yl) * block
            size = min(block, width - start)
            grad_ref[:, start : start + size] = total[:, :size] * scale
    value = grad_ref[...]
    norm = jnp.sum(value * value, axis=0, keepdims=True)
    row = lax.broadcasted_iota(jnp.int32, (rows, width), 0)
    small = jnp.where(row == rows - 1, norm, taps_ref[...]).astype(BF16)
    for member in range(GROUP):
        start = member * block
        size = min(block, width - start)
        for k in range(member * copies, (member + 1) * copies):
            small_ref[k, :, :size] = small[:, start : start + size]
            if size < block:
                small_ref[k, :, size:] = jnp.zeros((rows, block - size), BF16)


def chain_body(rows, *refs):
    *terms, gate_ref, up_ref, before_ref, after_ref, gate_taps, up_taps = refs[:10]
    gate_out, up_out, taps_out, gate_held, up_held, gate_back, up_back = refs[10:]
    reach = terms[0].shape[0]
    for at in range(0, gate_ref.shape[1], LANE):
        lanes = slice(at, at + LANE)

        def conv(which, source, taps, held):
            held[PAD - HALO : PAD] = before_ref[which, :, lanes].astype(F32)
            held[PAD : PAD + rows] = source[:, lanes].astype(F32)
            held[PAD + rows : PAD + rows + HALO] = after_ref[which, :, lanes].astype(F32)
            coef = [taps[k : k + 1, lanes].astype(F32) for k in range(3)]
            total = coef[2] * held[PAD : PAD + reach]
            for k in range(2):
                total += coef[k] * held[PAD - HALO + k : PAD - HALO + k + reach]
            return total, coef

        gate, gate_coef = conv(0, gate_ref, gate_taps, gate_held)
        up, up_coef = conv(1, up_ref, up_taps, up_held)
        d_hidden = terms[0][:, lanes].astype(F32)
        for term in terms[1:]:
            d_hidden += term[:, lanes].astype(F32)
        sig = 1.0 / (1.0 + jnp.exp(-gate))
        gate_back[...] = d_hidden * up * sig * (1.0 + gate * (1.0 - sig))
        up_back[...] = d_hidden * gate * sig

        def back(coef, held, out):
            total = coef[2] * held[:rows]
            for k in range(2):
                total += coef[k] * held[2 - k : 2 - k + rows]
            out[:, lanes] = total.astype(BF16)

        back(gate_coef, gate_back, gate_out)
        back(up_coef, up_back, up_out)
        for first, held, source in ((0, gate_back, gate_held), (3, up_back, up_held)):
            for k in range(3):
                start = PAD - HALO + k
                product = held[:rows] * source[start : start + rows]
                taps_out[first + k : first + k + 1, lanes] = jnp.sum(product, 0, keepdims=True)
        taps_out[6:, lanes] = jnp.zeros((2, LANE), F32)


def chain_of(terms, gate_pre, up_pre, before, after, gate_taps, up_taps, block):
    rows, width = gate_pre.shape
    reach = terms[0].shape[0]
    tall = pl.BlockSpec((reach, block), lambda i: (0, i))
    wide = pl.BlockSpec((rows, block), lambda i: (0, i))
    edge = pl.BlockSpec((2, HALO, block), lambda i: (0, 0, i))
    taps = pl.BlockSpec((3, block), lambda i: (0, i))
    grad = jax.ShapeDtypeStruct((rows, width), BF16)
    return call(
        functools.partial(chain_body, rows),
        (grad, grad, jax.ShapeDtypeStruct((8, width), F32)),
        flops=100 * rows * width,
        limit=60,
        grid=(GROUP,),
        in_specs=[tall] * 4 + [wide, wide, edge, edge, taps, taps],
        out_specs=(wide, wide, pl.BlockSpec((8, block), lambda i: (0, i))),
        scratch_shapes=[pltpu.VMEM((reach + PAD, LANE), F32)] * 2
        + [pltpu.VMEM((reach, LANE), F32)] * 2,
    )(*terms, gate_pre, up_pre, before, after, gate_taps, up_taps)


def total_of(seen_ref):
    total = None
    for source in range(seen_ref.shape[0]):
        part = seen_ref[source].astype(F32)
        total = part if total is None else total + part
    return total


def middle_body(seen_ref, small_ref):
    total = total_of(seen_ref).astype(small_ref.dtype)
    for k in range(small_ref.shape[0]):
        small_ref[k] = total


def last_body(scale, seen_ref, gate_ref, up_ref, norm_ref):
    block = seen_ref.shape[2]
    for member in range(GROUP):
        start = member * block
        size = min(block, gate_ref.shape[1] - start)
        lanes = slice(start, start + size)
        gate_ref[:, lanes] = seen_ref[member, :3, :size] * scale
        up_ref[:, lanes] = seen_ref[member, 3:6, :size] * scale
        norm_ref[:, lanes] = seen_ref[member, 7:, :size] / D


def local(gate_pre, up_pre, gate_taps, up_taps, down_weight, cotangent):
    rows, width = gate_pre.shape
    n_fs = lax.axis_size("fs")
    n_rep = lax.axis_size(ZY)
    n_near = lax.axis_size(NEAR)
    n_far = lax.axis_size(FAR)
    block = -(-(width // LANE) // GROUP) * LANE
    grad_scale = float(rows * n_rep * n_fs) ** (-0.5)

    before = passed_along(jnp.stack([gate_pre[-HALO:], up_pre[-HALO:]]), "fs", 1)
    after = passed_along(jnp.stack([gate_pre[:HALO], up_pre[:HALO]]), "fs", -1)

    axes = ("zl", "yl", "tp")
    first, second = [], []
    for i in range(8):
        flip = 4 if i % 2 == 0 else 2
        first.append((i, i ^ flip))
        if i % 2 == 0:
            second.append((i, i ^ 6))
    side = lax.ppermute(cotangent, axes, first)
    far = lax.ppermute(cotangent, axes, second)
    across = lax.ppermute(jnp.stack([side, far]), "tp", [(0, 1), (1, 0)])
    tp = lax.axis_index("tp")
    member = lax.axis_index("zl") * 2 + lax.axis_index("yl")
    order = jnp.stack(
        [member, member ^ (2 - tp), member ^ (1 + tp), member ^ 3]
    )

    turned = turn_of(tp[None], cotangent, side, far, across)

    hidden = hidden_of(gate_pre, up_pre, before, gate_taps, up_taps, block, n_fs)
    everyone = swap(hidden.reshape(n_near, rows, block), NEAR)

    me = lax.axis_index("fs")
    steps = (1, 3, 2, 0)
    hidden, cot_late = lax.optimization_barrier((hidden, cotangent))
    at = jnp.stack([(me + step) % n_fs for step in steps])
    terms = list(terms_of(at, cot_late, down_weight, rows))
    for k, step in enumerate(steps[:3]):
        pairs = [(i, (i + step) % n_fs) for i in range(n_fs)]
        terms[k] = lax.ppermute(terms[k], "fs", pairs)

    partial = grad_of(order, turned, everyone.reshape(GROUP, -1, block), n_rep)
    parts = swap(partial, ZY)

    grad_gate, grad_up, taps = chain_of(
        terms, gate_pre, up_pre, before, after, gate_taps, up_taps, block
    )

    sent = jax.ShapeDtypeStruct((n_near, 8, block), BF16)
    grad_share, small = call(
        functools.partial(share_body, grad_scale),
        (jax.ShapeDtypeStruct((8, width), F32), sent),
    )(parts, taps)
    small = call(middle_body, jax.ShapeDtypeStruct((n_far, 8, block), BF16))(swap(small, NEAR))
    small = call(middle_body, jax.ShapeDtypeStruct((GROUP, 8, block), F32))(swap(small, FAR))
    three = jax.ShapeDtypeStruct((3, width), F32)
    gate_out, up_out, norms = call(
        functools.partial(last_body, grad_scale),
        (three, three, jax.ShapeDtypeStruct((1, width), F32)),
    )(swap(small, ("zl", "yl")))
    return grad_gate, grad_up, gate_out, up_out, grad_share[None], norms[0]


def solution(mesh):
    finer = Mesh(
        mesh.devices.reshape(4, 2, 4, 2, mesh.shape["fs"], mesh.shape["tp"]),
        ("zh", "zl", "yh", "yl", "fs", "tp"),
    )
    in_specs = (P(TOK, "tp"), P(TOK, "tp"), P(None, "tp"), P(None, "tp"), P("tp", "fs"), P(ZY, "fs"))
    out_specs = (P(TOK, "tp"), P(TOK, "tp"), P(None, "tp"), P(None, "tp"), P("fs", ZY, "tp"), P("tp"))
    return jax.shard_map(local, mesh=finer, in_specs=in_specs, out_specs=out_specs, check_vma=False)
```

```python
import functools

import jax
import jax.numpy as jnp
from jax import lax
from jax.experimental import pallas as pl
from jax.experimental.pallas import tpu as pltpu
from jax.sharding import Mesh
from jax.sharding import PartitionSpec as P


D = 2048
ZY = ("zh", "zl", "yh", "yl")
TOK = ("zh", "zl", "yh", "yl", "fs")
NEAR = ("zl", "yl", "fs")
FAR = ("zh", "yh")
HALO = 2
PAD = 8
LANE = 128
GROUP = 4
F32 = jnp.float32
BF16 = jnp.bfloat16


def passed_along(array, axis, by):
    count = lax.axis_size(axis)
    pairs = [(i, i + by) for i in range(count) if 0 <= i + by < count]
    return lax.ppermute(array, axis, pairs)


def swap(array, axes):
    return lax.all_to_all(array, axes, 0, 0, tiled=True)


def mate(at, tp):
    return (at + (1 if (at + tp) % 2 == 0 else -1)) % 8


def groups_of(n_fs):
    groups = []
    for tp in range(2):
        for z in range(0, 8, 2):
            for y in range(0, 8, 2):
                places = [(i, j) for i in (z, mate(z, tp)) for j in (y, mate(y, tp))]
                groups.append(
                    [((i * 8 + j) * n_fs + x) * 2 + tp for i, j in places for x in range(n_fs)]
                )
    return groups


def call(body, out_shape, flops=0, limit=8, **kw):
    return pl.pallas_call(
        body,
        out_shape=out_shape,
        compiler_params=pltpu.CompilerParams(vmem_limit_bytes=limit << 20),
        cost_estimate=pl.CostEstimate(flops=flops, bytes_accessed=1 << 20, transcendentals=0),
        **kw,
    )


def hidden_body(rows, width, gate_ref, up_ref, before_ref, gate_taps, up_taps, out_ref, held_ref):
    step = pl.program_id(0)
    block = gate_ref.shape[1]

    def conv(which, source, taps):
        held_ref[PAD - HALO : PAD] = before_ref[which].astype(F32)
        held_ref[PAD : PAD + rows] = source[...].astype(F32)
        total = taps[2:3].astype(F32) * held_ref[PAD : PAD + rows]
        for k in range(2):
            start = PAD - HALO + k
            total += taps[k : k + 1].astype(F32) * held_ref[start : start + rows]
        return total

    gate = conv(0, gate_ref, gate_taps)
    up = conv(1, up_ref, up_taps)
    value = gate * (1.0 / (1.0 + jnp.exp(-gate))) * up
    lane = lax.broadcasted_iota(jnp.int32, value.shape, 1) + step * block
    value = jnp.where(lane < width, value, 0.0).astype(BF16)
    for k in range(out_ref.shape[1]):
        out_ref[0, k] = value


def hidden_of(gate_pre, up_pre, before, gate_taps, up_taps, block, n_fs):
    rows, width = gate_pre.shape
    wide = pl.BlockSpec((rows, block), lambda i: (0, i))
    taps = pl.BlockSpec((3, block), lambda i: (0, i))
    return call(
        functools.partial(hidden_body, rows, width),
        jax.ShapeDtypeStruct((GROUP, n_fs, rows, block), BF16),
        flops=40 * rows * width,
        limit=60,
        grid=(GROUP,),
        in_specs=[wide, wide, pl.BlockSpec((2, HALO, block), lambda i: (0, 0, i)), taps, taps],
        out_specs=pl.BlockSpec((1, n_fs, rows, block), lambda i: (i, 0, 0, 0)),
        scratch_shapes=[pltpu.VMEM((rows + PAD, block), F32)],
    )(gate_pre, up_pre, before, gate_taps, up_taps)


def terms_body(rows, at_ref, cot_ref, weight_ref, *refs):
    *outs, held_ref = refs
    tokens = cot_ref.shape[0]
    held_ref[:tokens] = cot_ref[...]
    held_ref[tokens:] = jnp.zeros((held_ref.shape[0] - tokens, held_ref.shape[1]), BF16)
    for k, out in enumerate(outs):
        start = pl.multiple_of(at_ref[k] * rows, 16)
        out[...] = lax.dot_general(
            held_ref[pl.ds(start, rows + PAD)],
            weight_ref[...],
            (((1,), (1,)), ((), ())),
            preferred_element_type=F32,
        ).astype(BF16)


def terms_of(at, cotangent, weight, rows):
    tokens, depth = cotangent.shape
    width = weight.shape[0]
    whole = pl.BlockSpec(memory_space=pltpu.VMEM)
    steps = tokens // rows
    return call(
        functools.partial(terms_body, rows),
        (jax.ShapeDtypeStruct((rows + PAD, width), BF16),) * steps,
        flops=2 * tokens * depth * width,
        limit=16,
        in_specs=[pl.BlockSpec(memory_space=pltpu.SMEM), whole, whole],
        out_specs=(whole,) * steps,
        scratch_shapes=[pltpu.VMEM((tokens + 2 * PAD, depth), BF16)],
    )(at, cotangent, weight)


def order_body(order_ref, out_ref):
    for k in range(GROUP):
        out_ref[k] = order_ref[k]


def order_of(order):
    scalars = pl.BlockSpec(memory_space=pltpu.SMEM)
    return call(
        order_body,
        jax.ShapeDtypeStruct(order.shape, order.dtype),
        in_specs=[scalars],
        out_specs=scalars,
    )(order)


def grad_body(order_ref, *refs):
    blocks, hidden = refs[:GROUP], refs[GROUP]
    out_ref, cot_ref, rows_ref, cot_sem, row_sem = refs[GROUP + 1 :]
    tokens = hidden.shape[1]

    def fetch(k):
        return pltpu.make_async_copy(
            blocks[k], cot_ref.at[pl.ds(k * tokens, tokens)], cot_sem.at[k]
        )

    def fetch_rows(k):
        return pltpu.make_async_copy(
            hidden.at[order_ref[k]], rows_ref.at[pl.ds(k * tokens, tokens)], row_sem.at[k]
        )

    for k in range(GROUP):
        fetch(k).start()
        fetch_rows(k).start()
    total = None
    for part in range(2):
        for k in (2 * part, 2 * part + 1):
            fetch(k).wait()
            fetch_rows(k).wait()
        span = slice(2 * part * tokens, 2 * (part + 1) * tokens)
        value = lax.dot_general(
            cot_ref[span], rows_ref[span], (((0,), (0,)), ((), ())), preferred_element_type=F32
        )
        total = value if total is None else total + value
    out_ref[...] = total.astype(BF16).reshape(out_ref.shape)


def grad_of(order, blocks, hidden, n_rep):
    tokens, depth = blocks[0].shape
    block = hidden.shape[2]
    return call(
        grad_body,
        jax.ShapeDtypeStruct((n_rep, depth // n_rep, block), BF16),
        flops=2 * GROUP * tokens * depth * block,
        limit=60,
        in_specs=[pl.BlockSpec(memory_space=pltpu.SMEM)]
        + [pl.BlockSpec(memory_space=pl.ANY)] * (GROUP + 1),
        out_specs=pl.BlockSpec(memory_space=pltpu.VMEM),
        scratch_shapes=[
            pltpu.VMEM((GROUP * tokens, depth), BF16),
            pltpu.VMEM((GROUP * tokens, block), BF16),
            pltpu.SemaphoreType.DMA((GROUP,)),
            pltpu.SemaphoreType.DMA((GROUP,)),
        ],
    )(order, *blocks, hidden)


def share_body(scale, parts_ref, taps_ref, grad_ref, small_ref):
    block = parts_ref.shape[2]
    rows, width = taps_ref.shape
    copies = small_ref.shape[0] // GROUP
    for zl in range(2):
        for yl in range(2):
            total = None
            for zh in range(4):
                for yh in range(4):
                    part = parts_ref[((zh * 2 + zl) * 4 + yh) * 2 + yl].astype(F32)
                    total = part if total is None else total + part
            start = (zl * 2 + yl) * block
            size = min(block, width - start)
            grad_ref[:, start : start + size] = total[:, :size] * scale
    value = grad_ref[...]
    norm = jnp.sum(value * value, axis=0, keepdims=True)
    row = lax.broadcasted_iota(jnp.int32, (rows, width), 0)
    small = jnp.where(row == rows - 1, norm, taps_ref[...]).astype(BF16)
    for member in range(GROUP):
        start = member * block
        size = min(block, width - start)
        for k in range(member * copies, (member + 1) * copies):
            small_ref[k, :, :size] = small[:, start : start + size]
            if size < block:
                small_ref[k, :, size:] = jnp.zeros((rows, block - size), BF16)


def chain_body(rows, *refs):
    *terms, gate_ref, up_ref, before_ref, after_ref, gate_taps, up_taps = refs[:10]
    gate_out, up_out, taps_out, gate_held, up_held, gate_back, up_back = refs[10:]
    reach = terms[0].shape[0]
    for at in range(0, gate_ref.shape[1], LANE):
        lanes = slice(at, at + LANE)

        def conv(which, source, taps, held):
            held[PAD - HALO : PAD] = before_ref[which, :, lanes].astype(F32)
            held[PAD : PAD + rows] = source[:, lanes].astype(F32)
            held[PAD + rows : PAD + rows + HALO] = after_ref[which, :, lanes].astype(F32)
            coef = [taps[k : k + 1, lanes].astype(F32) for k in range(3)]
            total = coef[2] * held[PAD : PAD + reach]
            for k in range(2):
                total += coef[k] * held[PAD - HALO + k : PAD - HALO + k + reach]
            return total, coef

        gate, gate_coef = conv(0, gate_ref, gate_taps, gate_held)
        up, up_coef = conv(1, up_ref, up_taps, up_held)
        d_hidden = terms[0][:, lanes].astype(F32)
        for term in terms[1:]:
            d_hidden += term[:, lanes].astype(F32)
        sig = 1.0 / (1.0 + jnp.exp(-gate))
        gate_back[...] = d_hidden * up * sig * (1.0 + gate * (1.0 - sig))
        up_back[...] = d_hidden * gate * sig

        def back(coef, held, out):
            total = coef[2] * held[:rows]
            for k in range(2):
                total += coef[k] * held[2 - k : 2 - k + rows]
            out[:, lanes] = total.astype(BF16)

        back(gate_coef, gate_back, gate_out)
        back(up_coef, up_back, up_out)
        for first, held, source in ((0, gate_back, gate_held), (3, up_back, up_held)):
            for k in range(3):
                start = PAD - HALO + k
                product = held[:rows] * source[start : start + rows]
                taps_out[first + k : first + k + 1, lanes] = jnp.sum(product, 0, keepdims=True)
        taps_out[6:, lanes] = jnp.zeros((2, LANE), F32)


def chain_of(terms, gate_pre, up_pre, before, after, gate_taps, up_taps, block):
    rows, width = gate_pre.shape
    reach = terms[0].shape[0]
    tall = pl.BlockSpec((reach, block), lambda i: (0, i))
    wide = pl.BlockSpec((rows, block), lambda i: (0, i))
    edge = pl.BlockSpec((2, HALO, block), lambda i: (0, 0, i))
    taps = pl.BlockSpec((3, block), lambda i: (0, i))
    grad = jax.ShapeDtypeStruct((rows, width), BF16)
    return call(
        functools.partial(chain_body, rows),
        (grad, grad, jax.ShapeDtypeStruct((8, width), F32)),
        flops=100 * rows * width,
        limit=60,
        grid=(GROUP,),
        in_specs=[tall] * 4 + [wide, wide, edge, edge, taps, taps],
        out_specs=(wide, wide, pl.BlockSpec((8, block), lambda i: (0, i))),
        scratch_shapes=[pltpu.VMEM((reach + PAD, LANE), F32)] * 2
        + [pltpu.VMEM((reach, LANE), F32)] * 2,
    )(*terms, gate_pre, up_pre, before, after, gate_taps, up_taps)


def total_of(seen_ref):
    total = None
    for source in range(seen_ref.shape[0]):
        part = seen_ref[source].astype(F32)
        total = part if total is None else total + part
    return total


def middle_body(seen_ref, small_ref):
    total = total_of(seen_ref).astype(small_ref.dtype)
    for k in range(small_ref.shape[0]):
        small_ref[k] = total


def last_body(scale, seen_ref, gate_ref, up_ref, norm_ref):
    block = seen_ref.shape[2]
    for member in range(GROUP):
        start = member * block
        size = min(block, gate_ref.shape[1] - start)
        lanes = slice(start, start + size)
        gate_ref[:, lanes] = seen_ref[member, :3, :size] * scale
        up_ref[:, lanes] = seen_ref[member, 3:6, :size] * scale
        norm_ref[:, lanes] = seen_ref[member, 7:, :size] / D


def local(gate_pre, up_pre, gate_taps, up_taps, down_weight, cotangent):
    rows, width = gate_pre.shape
    n_fs = lax.axis_size("fs")
    n_rep = lax.axis_size(ZY)
    n_near = lax.axis_size(NEAR)
    n_far = lax.axis_size(FAR)
    block = -(-(width // LANE) // GROUP) * LANE
    grad_scale = float(rows * n_rep * n_fs) ** (-0.5)

    before = passed_along(jnp.stack([gate_pre[-HALO:], up_pre[-HALO:]]), "fs", 1)
    after = passed_along(jnp.stack([gate_pre[:HALO], up_pre[:HALO]]), "fs", -1)

    def collected(flip_z, flip_y):
        pairs = []
        for z in range(8):
            for y in range(8):
                for tp in range(2):
                    to_z = mate(z, tp) if flip_z else z
                    to_y = mate(y, tp) if flip_y else y
                    pairs.append(((z * 8 + y) * 2 + tp, (to_z * 8 + to_y) * 2 + tp))
        return lax.ppermute(cotangent, ZY + ("tp",), pairs)

    blocks = [cotangent, collected(True, False)]
    blocks.append(collected(False, True))
    blocks.append(collected(True, True))
    member = lax.axis_index("zl") * 2 + lax.axis_index("yl")
    order = order_of(jnp.stack([member, member ^ 2, member ^ 1, member ^ 3]))

    hidden = hidden_of(gate_pre, up_pre, before, gate_taps, up_taps, block, n_fs)
    everyone = lax.all_to_all(
        hidden.reshape(n_near, rows, block),
        TOK + ("tp",),
        0,
        0,
        tiled=True,
        axis_index_groups=groups_of(n_fs),
    )

    me = lax.axis_index("fs")
    steps = (1, 3, 2, 0)
    hidden, cot_late = lax.optimization_barrier((hidden, cotangent))
    at = jnp.stack([(me + step) % n_fs for step in steps])
    terms = list(terms_of(at, cot_late, down_weight, rows))
    for k, step in enumerate(steps[:3]):
        pairs = [(i, (i + step) % n_fs) for i in range(n_fs)]
        terms[k] = lax.ppermute(terms[k], "fs", pairs)

    partial = grad_of(order, blocks, everyone.reshape(GROUP, -1, block), n_rep)
    parts = swap(partial, ZY)

    grad_gate, grad_up, taps = chain_of(
        terms, gate_pre, up_pre, before, after, gate_taps, up_taps, block
    )

    sent = jax.ShapeDtypeStruct((n_near, 8, block), BF16)
    grad_share, small = call(
        functools.partial(share_body, grad_scale), (jax.ShapeDtypeStruct((8, width), F32), sent)
    )(parts, taps)
    small = call(middle_body, jax.ShapeDtypeStruct((n_far, 8, block), BF16))(swap(small, NEAR))
    small = call(middle_body, jax.ShapeDtypeStruct((GROUP, 8, block), F32))(swap(small, FAR))
    three = jax.ShapeDtypeStruct((3, width), F32)
    gate_out, up_out, norms = call(
        functools.partial(last_body, grad_scale),
        (three, three, jax.ShapeDtypeStruct((1, width), F32)),
    )(swap(small, ("zl", "yl")))
    return grad_gate, grad_up, gate_out, up_out, grad_share[None], norms[0]


def solution(mesh):
    finer = Mesh(
        mesh.devices.reshape(4, 2, 4, 2, mesh.shape["fs"], mesh.shape["tp"]),
        ("zh", "zl", "yh", "yl", "fs", "tp"),
    )
    in_specs = (P(TOK, "tp"), P(TOK, "tp"), P(None, "tp"), P(None, "tp"), P("tp", "fs"), P(ZY, "fs"))
    out_specs = (P(TOK, "tp"), P(TOK, "tp"), P(None, "tp"), P(None, "tp"), P("fs", ZY, "tp"), P("tp"))
    return jax.shard_map(local, mesh=finer, in_specs=in_specs, out_specs=out_specs, check_vma=False)
```

```python
import functools

import jax
import jax.numpy as jnp
from jax import lax
from jax.experimental import pallas as pl
from jax.experimental.pallas import tpu as pltpu
from jax.sharding import Mesh
from jax.sharding import PartitionSpec as P


D = 2048
ZY = ("zh", "zl", "yh", "yl")
TOK = ("zh", "zl", "yh", "yl", "fs")
NEAR = ("zl", "yl", "fs")
FAR = ("zh", "yh")
HALO = 2
PAD = 8
LANE = 128
GROUP = 4
F32 = jnp.float32
BF16 = jnp.bfloat16


def passed_along(array, axis, by):
    count = lax.axis_size(axis)
    pairs = [(i, i + by) for i in range(count) if 0 <= i + by < count]
    return lax.ppermute(array, axis, pairs)


def swap(array, axes):
    return lax.all_to_all(array, axes, 0, 0, tiled=True)


def mate(at, tp):
    return (at + (1 if (at + tp) % 2 == 0 else -1)) % 8


def groups_of(n_fs):
    groups = []
    for tp in range(2):
        for z in range(0, 8, 2):
            for y in range(0, 8, 2):
                places = [(i, j) for i in (z, mate(z, tp)) for j in (y, mate(y, tp))]
                groups.append(
                    [((i * 8 + j) * n_fs + x) * 2 + tp for i, j in places for x in range(n_fs)]
                )
    return groups


def call(body, out_shape, flops=0, limit=8, **kw):
    return pl.pallas_call(
        body,
        out_shape=out_shape,
        compiler_params=pltpu.CompilerParams(vmem_limit_bytes=limit << 20),
        cost_estimate=pl.CostEstimate(flops=flops, bytes_accessed=1 << 20, transcendentals=0),
        **kw,
    )


def hidden_body(rows, width, gate_ref, up_ref, before_ref, gate_taps, up_taps, out_ref, held_ref):
    step = pl.program_id(0)
    block = gate_ref.shape[1]

    def conv(which, source, taps, lanes):
        held_ref[which, PAD - HALO : PAD] = before_ref[which, :, lanes].astype(F32)
        held_ref[which, PAD : PAD + rows] = source[:, lanes].astype(F32)
        total = taps[2:3, lanes].astype(F32) * held_ref[which, PAD : PAD + rows]
        for k in range(2):
            start = PAD - HALO + k
            total += taps[k : k + 1, lanes].astype(F32) * held_ref[which, start : start + rows]
        return total

    for at in range(0, block, LANE):
        lanes = slice(at, at + LANE)
        gate = conv(0, gate_ref, gate_taps, lanes)
        up = conv(1, up_ref, up_taps, lanes)
        value = gate * (1.0 / (1.0 + jnp.exp(-gate))) * up
        value = jnp.where(step * block + at < width, value, 0.0).astype(BF16)
        for k in range(out_ref.shape[1]):
            out_ref[0, k, :, lanes] = value


def hidden_of(gate_pre, up_pre, before, gate_taps, up_taps, block, n_fs):
    rows, width = gate_pre.shape
    wide = pl.BlockSpec((rows, block), lambda i: (0, i))
    taps = pl.BlockSpec((3, block), lambda i: (0, i))
    return call(
        functools.partial(hidden_body, rows, width),
        jax.ShapeDtypeStruct((GROUP, n_fs, rows, block), BF16),
        flops=40 * rows * width,
        limit=62,
        grid=(GROUP,),
        in_specs=[wide, wide, pl.BlockSpec((2, HALO, block), lambda i: (0, 0, i)), taps, taps],
        out_specs=pl.BlockSpec((1, n_fs, rows, block), lambda i: (i, 0, 0, 0)),
        scratch_shapes=[pltpu.VMEM((2, rows + PAD, LANE), F32)],
    )(gate_pre, up_pre, before, gate_taps, up_taps)


def terms_body(rows, at_ref, cot_ref, weight_ref, *refs):
    *outs, held_ref = refs
    tokens = cot_ref.shape[0]
    held_ref[:tokens] = cot_ref[...]
    held_ref[tokens:] = jnp.zeros((held_ref.shape[0] - tokens, held_ref.shape[1]), BF16)
    for k, out in enumerate(outs):
        start = pl.multiple_of(at_ref[k] * rows, 16)
        out[...] = lax.dot_general(
            held_ref[pl.ds(start, rows + PAD)],
            weight_ref[...],
            (((1,), (1,)), ((), ())),
            preferred_element_type=F32,
        ).astype(BF16)


def terms_of(at, cotangent, weight, rows):
    tokens, depth = cotangent.shape
    width = weight.shape[0]
    whole = pl.BlockSpec(memory_space=pltpu.VMEM)
    steps = tokens // rows
    return call(
        functools.partial(terms_body, rows),
        (jax.ShapeDtypeStruct((rows + PAD, width), BF16),) * steps,
        flops=2 * tokens * depth * width,
        limit=16,
        in_specs=[pl.BlockSpec(memory_space=pltpu.SMEM), whole, whole],
        out_specs=(whole,) * steps,
        scratch_shapes=[pltpu.VMEM((tokens + 2 * PAD, depth), BF16)],
    )(at, cotangent, weight)


def order_body(order_ref, out_ref):
    for k in range(GROUP):
        out_ref[k] = order_ref[k]


def order_of(order):
    scalars = pl.BlockSpec(memory_space=pltpu.SMEM)
    return call(
        order_body,
        jax.ShapeDtypeStruct(order.shape, order.dtype),
        in_specs=[scalars],
        out_specs=scalars,
    )(order)


def grad_body(order_ref, *refs):
    blocks, hidden = refs[:GROUP], refs[GROUP]
    out_ref, cot_ref, rows_ref, cot_sem, row_sem = refs[GROUP + 1 :]
    tokens = hidden.shape[1]

    def fetch(k):
        return pltpu.make_async_copy(
            blocks[k], cot_ref.at[pl.ds(k * tokens, tokens)], cot_sem.at[k]
        )

    def fetch_rows(k):
        return pltpu.make_async_copy(
            hidden.at[order_ref[k]], rows_ref.at[pl.ds(k * tokens, tokens)], row_sem.at[k]
        )

    for k in range(GROUP):
        fetch(k).start()
        fetch_rows(k).start()
    total = None
    for k in range(GROUP):
        fetch(k).wait()
        fetch_rows(k).wait()
        span = slice(k * tokens, (k + 1) * tokens)
        value = lax.dot_general(
            cot_ref[span], rows_ref[span], (((0,), (0,)), ((), ())), preferred_element_type=F32
        )
        total = value if total is None else total + value
    out_ref[...] = total.astype(BF16).reshape(out_ref.shape)


def grad_of(order, blocks, hidden, n_rep):
    tokens, depth = blocks[0].shape
    block = hidden.shape[2]
    return call(
        grad_body,
        jax.ShapeDtypeStruct((n_rep, depth // n_rep, block), BF16),
        flops=2 * GROUP * tokens * depth * block,
        limit=62,
        in_specs=[pl.BlockSpec(memory_space=pltpu.SMEM)]
        + [pl.BlockSpec(memory_space=pl.ANY)] * (GROUP + 1),
        out_specs=pl.BlockSpec(memory_space=pltpu.VMEM),
        scratch_shapes=[
            pltpu.VMEM((GROUP * tokens, depth), BF16),
            pltpu.VMEM((GROUP * tokens, block), BF16),
            pltpu.SemaphoreType.DMA((GROUP,)),
            pltpu.SemaphoreType.DMA((GROUP,)),
        ],
    )(order, *blocks, hidden)


def share_body(scale, parts_ref, taps_ref, grad_ref, small_ref):
    block = parts_ref.shape[2]
    rows, width = taps_ref.shape
    copies = small_ref.shape[0] // GROUP
    for zl in range(2):
        for yl in range(2):
            total = None
            for zh in range(4):
                for yh in range(4):
                    part = parts_ref[((zh * 2 + zl) * 4 + yh) * 2 + yl].astype(F32)
                    total = part if total is None else total + part
            start = (zl * 2 + yl) * block
            size = min(block, width - start)
            grad_ref[:, start : start + size] = total[:, :size] * scale
    value = grad_ref[...]
    norm = jnp.sum(value * value, axis=0, keepdims=True)
    row = lax.broadcasted_iota(jnp.int32, (rows, width), 0)
    small = jnp.where(row == rows - 1, norm, taps_ref[...]).astype(BF16)
    for member in range(GROUP):
        start = member * block
        size = min(block, width - start)
        for k in range(member * copies, (member + 1) * copies):
            small_ref[k, :, :size] = small[:, start : start + size]
            if size < block:
                small_ref[k, :, size:] = jnp.zeros((rows, block - size), BF16)


def chain_body(rows, *refs):
    *terms, gate_ref, up_ref, before_ref, after_ref, gate_taps, up_taps = refs[:10]
    gate_out, up_out, taps_out, gate_held, up_held, gate_back, up_back = refs[10:]
    reach = terms[0].shape[0]
    for at in range(0, gate_ref.shape[1], LANE):
        lanes = slice(at, at + LANE)

        def conv(which, source, taps, held):
            held[PAD - HALO : PAD] = before_ref[which, :, lanes].astype(F32)
            held[PAD : PAD + rows] = source[:, lanes].astype(F32)
            held[PAD + rows : PAD + rows + HALO] = after_ref[which, :, lanes].astype(F32)
            coef = [taps[k : k + 1, lanes].astype(F32) for k in range(3)]
            total = coef[2] * held[PAD : PAD + reach]
            for k in range(2):
                total += coef[k] * held[PAD - HALO + k : PAD - HALO + k + reach]
            return total, coef

        gate, gate_coef = conv(0, gate_ref, gate_taps, gate_held)
        up, up_coef = conv(1, up_ref, up_taps, up_held)
        d_hidden = terms[0][:, lanes].astype(F32)
        for term in terms[1:]:
            d_hidden += term[:, lanes].astype(F32)
        sig = 1.0 / (1.0 + jnp.exp(-gate))
        gate_back[...] = d_hidden * up * sig * (1.0 + gate * (1.0 - sig))
        up_back[...] = d_hidden * gate * sig

        def back(coef, held, out):
            total = coef[2] * held[:rows]
            for k in range(2):
                total += coef[k] * held[2 - k : 2 - k + rows]
            out[:, lanes] = total.astype(BF16)

        back(gate_coef, gate_back, gate_out)
        back(up_coef, up_back, up_out)
        for first, held, source in ((0, gate_back, gate_held), (3, up_back, up_held)):
            for k in range(3):
                start = PAD - HALO + k
                product = held[:rows] * source[start : start + rows]
                taps_out[first + k : first + k + 1, lanes] = jnp.sum(product, 0, keepdims=True)
        taps_out[6:, lanes] = jnp.zeros((2, LANE), F32)


def chain_of(terms, gate_pre, up_pre, before, after, gate_taps, up_taps, block):
    rows, width = gate_pre.shape
    reach = terms[0].shape[0]
    tall = pl.BlockSpec((reach, block), lambda i: (0, i))
    wide = pl.BlockSpec((rows, block), lambda i: (0, i))
    edge = pl.BlockSpec((2, HALO, block), lambda i: (0, 0, i))
    taps = pl.BlockSpec((3, block), lambda i: (0, i))
    grad = jax.ShapeDtypeStruct((rows, width), BF16)
    return call(
        functools.partial(chain_body, rows),
        (grad, grad, jax.ShapeDtypeStruct((8, width), F32)),
        flops=100 * rows * width,
        limit=62,
        grid=(GROUP,),
        in_specs=[tall] * 4 + [wide, wide, edge, edge, taps, taps],
        out_specs=(wide, wide, pl.BlockSpec((8, block), lambda i: (0, i))),
        scratch_shapes=[pltpu.VMEM((reach + PAD, LANE), F32)] * 2
        + [pltpu.VMEM((reach, LANE), F32)] * 2,
    )(*terms, gate_pre, up_pre, before, after, gate_taps, up_taps)


def total_of(seen_ref):
    total = None
    for source in range(seen_ref.shape[0]):
        part = seen_ref[source].astype(F32)
        total = part if total is None else total + part
    return total


def middle_body(seen_ref, small_ref):
    total = total_of(seen_ref).astype(small_ref.dtype)
    for k in range(small_ref.shape[0]):
        small_ref[k] = total


def last_body(scale, seen_ref, gate_ref, up_ref, norm_ref):
    block = seen_ref.shape[2]
    for member in range(GROUP):
        start = member * block
        size = min(block, gate_ref.shape[1] - start)
        lanes = slice(start, start + size)
        gate_ref[:, lanes] = seen_ref[member, :3, :size] * scale
        up_ref[:, lanes] = seen_ref[member, 3:6, :size] * scale
        norm_ref[lanes] = seen_ref[member, 7, :size] / D


def local(gate_pre, up_pre, gate_taps, up_taps, down_weight, cotangent):
    rows, width = gate_pre.shape
    n_fs = lax.axis_size("fs")
    n_rep = lax.axis_size(ZY)
    n_near = lax.axis_size(NEAR)
    n_far = lax.axis_size(FAR)
    block = -(-(width // LANE) // GROUP) * LANE
    grad_scale = float(rows * n_rep * n_fs) ** (-0.5)

    before = passed_along(jnp.stack([gate_pre[-HALO:], up_pre[-HALO:]]), "fs", 1)
    after = passed_along(jnp.stack([gate_pre[:HALO], up_pre[:HALO]]), "fs", -1)

    def collected(flip_z, flip_y):
        pairs = []
        for z in range(8):
            for y in range(8):
                for tp in range(2):
                    to_z = mate(z, tp) if flip_z else z
                    to_y = mate(y, tp) if flip_y else y
                    pairs.append(((z * 8 + y) * 2 + tp, (to_z * 8 + to_y) * 2 + tp))
        return lax.ppermute(cotangent, ZY + ("tp",), pairs)

    blocks = [cotangent, collected(True, False)]
    blocks.append(collected(False, True))
    blocks.append(collected(True, True))
    member = lax.axis_index("zl") * 2 + lax.axis_index("yl")
    order = order_of(jnp.stack([member, member ^ 2, member ^ 1, member ^ 3]))

    hidden = hidden_of(gate_pre, up_pre, before, gate_taps, up_taps, block, n_fs)
    everyone = lax.all_to_all(
        hidden.reshape(n_near, rows, block),
        TOK + ("tp",),
        0,
        0,
        tiled=True,
        axis_index_groups=groups_of(n_fs),
    )

    me = lax.axis_index("fs")
    steps = (1, 3, 2, 0)
    hidden, cot_late = lax.optimization_barrier((hidden, cotangent))
    at = jnp.stack([(me + step) % n_fs for step in steps])
    terms = list(terms_of(at, cot_late, down_weight, rows))
    for k, step in enumerate(steps[:3]):
        pairs = [(i, (i + step) % n_fs) for i in range(n_fs)]
        terms[k] = lax.ppermute(terms[k], "fs", pairs)

    partial = grad_of(order, blocks, everyone.reshape(GROUP, -1, block), n_rep)
    parts = swap(partial, ZY)

    grad_gate, grad_up, taps = chain_of(
        terms, gate_pre, up_pre, before, after, gate_taps, up_taps, block
    )

    sent = jax.ShapeDtypeStruct((n_near, 8, block), BF16)
    grad_share, small = call(
        functools.partial(share_body, grad_scale), (jax.ShapeDtypeStruct((8, width), F32), sent)
    )(parts, taps)
    small = call(middle_body, jax.ShapeDtypeStruct((n_far, 8, block), BF16))(swap(small, NEAR))
    small = call(middle_body, jax.ShapeDtypeStruct((GROUP, 8, block), F32))(swap(small, FAR))
    three = jax.ShapeDtypeStruct((3, width), F32)
    gate_out, up_out, norms = call(
        functools.partial(last_body, grad_scale),
        (three, three, jax.ShapeDtypeStruct((width,), F32)),
    )(swap(small, ("zl", "yl")))
    return grad_gate, grad_up, gate_out, up_out, grad_share[None], norms


def solution(mesh):
    finer = Mesh(
        mesh.devices.reshape(4, 2, 4, 2, mesh.shape["fs"], mesh.shape["tp"]),
        ("zh", "zl", "yh", "yl", "fs", "tp"),
    )
    in_specs = (P(TOK, "tp"), P(TOK, "tp"), P(None, "tp"), P(None, "tp"), P("tp", "fs"), P(ZY, "fs"))
    out_specs = (P(TOK, "tp"), P(TOK, "tp"), P(None, "tp"), P(None, "tp"), P("fs", ZY, "tp"), P("tp"))
    return jax.shard_map(local, mesh=finer, in_specs=in_specs, out_specs=out_specs, check_vma=False)
```

```python
import functools

import jax
import jax.numpy as jnp
from jax import lax
from jax.experimental import pallas as pl
from jax.experimental.pallas import tpu as pltpu
from jax.sharding import Mesh
from jax.sharding import PartitionSpec as P


D = 2048
ZY = ("zh", "zl", "yh", "yl")
TOK = ("zh", "zl", "yh", "yl", "fs")
NEAR = ("zl", "yl", "fs")
FAR = ("zh", "yh")
HALO = 2
PAD = 8
LANE = 128
GROUP = 4
F32 = jnp.float32
BF16 = jnp.bfloat16


def passed_along(array, axis, by):
    count = lax.axis_size(axis)
    pairs = [(i, i + by) for i in range(count) if 0 <= i + by < count]
    return lax.ppermute(array, axis, pairs)


def swap(array, axes):
    return lax.all_to_all(array, axes, 0, 0, tiled=True)


def mate(at, tp):
    return (at + (1 if (at + tp) % 2 == 0 else -1)) % 8


def groups_of(n_fs):
    groups = []
    for tp in range(2):
        for z in range(0, 8, 2):
            for y in range(0, 8, 2):
                places = [(i, j) for i in (z, mate(z, tp)) for j in (y, mate(y, tp))]
                groups.append(
                    [((i * 8 + j) * n_fs + x) * 2 + tp for i, j in places for x in range(n_fs)]
                )
    return groups


def call(body, out_shape, flops=0, limit=8, **kw):
    return pl.pallas_call(
        body,
        out_shape=out_shape,
        compiler_params=pltpu.CompilerParams(vmem_limit_bytes=limit << 20),
        cost_estimate=pl.CostEstimate(flops=flops, bytes_accessed=1 << 20, transcendentals=0),
        **kw,
    )


def hidden_body(rows, width, gate_ref, up_ref, before_ref, gate_taps, up_taps, out_ref, held_ref):
    step = pl.program_id(0)
    block = gate_ref.shape[1]

    def conv(which, source, taps, lanes):
        held_ref[which, PAD - HALO : PAD] = before_ref[which, :, lanes].astype(F32)
        held_ref[which, PAD : PAD + rows] = source[:, lanes].astype(F32)
        total = taps[2:3, lanes].astype(F32) * held_ref[which, PAD : PAD + rows]
        for k in range(2):
            start = PAD - HALO + k
            total += taps[k : k + 1, lanes].astype(F32) * held_ref[which, start : start + rows]
        return total

    for at in range(0, block, LANE):
        lanes = slice(at, at + LANE)
        gate = conv(0, gate_ref, gate_taps, lanes)
        up = conv(1, up_ref, up_taps, lanes)
        value = gate * (1.0 / (1.0 + jnp.exp(-gate))) * up
        value = jnp.where(step * block + at < width, value, 0.0).astype(BF16)
        for k in range(out_ref.shape[1]):
            out_ref[0, k, :, lanes] = value


def hidden_of(gate_pre, up_pre, before, gate_taps, up_taps, block, n_fs):
    rows, width = gate_pre.shape
    wide = pl.BlockSpec((rows, block), lambda i: (0, i))
    taps = pl.BlockSpec((3, block), lambda i: (0, i))
    return call(
        functools.partial(hidden_body, rows, width),
        jax.ShapeDtypeStruct((GROUP, n_fs, rows, block), BF16),
        flops=40 * rows * width,
        limit=62,
        grid=(GROUP,),
        in_specs=[wide, wide, pl.BlockSpec((2, HALO, block), lambda i: (0, 0, i)), taps, taps],
        out_specs=pl.BlockSpec((1, n_fs, rows, block), lambda i: (i, 0, 0, 0)),
        scratch_shapes=[pltpu.VMEM((2, rows + PAD, LANE), F32)],
    )(gate_pre, up_pre, before, gate_taps, up_taps)


def terms_body(rows, at_ref, cot_ref, weight_ref, *refs):
    *outs, held_ref = refs
    tokens = cot_ref.shape[0]
    held_ref[:tokens] = cot_ref[...]
    held_ref[tokens:] = jnp.zeros((held_ref.shape[0] - tokens, held_ref.shape[1]), BF16)
    for k, out in enumerate(outs):
        start = pl.multiple_of(at_ref[k] * rows, 16)
        out[...] = lax.dot_general(
            held_ref[pl.ds(start, rows + PAD)],
            weight_ref[...],
            (((1,), (1,)), ((), ())),
            preferred_element_type=F32,
        ).astype(BF16)


def terms_of(at, cotangent, weight, rows):
    tokens, depth = cotangent.shape
    width = weight.shape[0]
    whole = pl.BlockSpec(memory_space=pltpu.VMEM)
    steps = tokens // rows
    return call(
        functools.partial(terms_body, rows),
        (jax.ShapeDtypeStruct((rows + PAD, width), BF16),) * steps,
        flops=2 * tokens * depth * width,
        limit=16,
        in_specs=[pl.BlockSpec(memory_space=pltpu.SMEM), whole, whole],
        out_specs=(whole,) * steps,
        scratch_shapes=[pltpu.VMEM((tokens + 2 * PAD, depth), BF16)],
    )(at, cotangent, weight)


def order_body(order_ref, out_ref):
    for k in range(GROUP):
        out_ref[k] = order_ref[k]


def order_of(order):
    scalars = pl.BlockSpec(memory_space=pltpu.SMEM)
    return call(
        order_body,
        jax.ShapeDtypeStruct(order.shape, order.dtype),
        in_specs=[scalars],
        out_specs=scalars,
    )(order)


def grad_body(order_ref, *refs):
    blocks, hidden = refs[:GROUP], refs[GROUP]
    out_ref, cot_ref, rows_ref, cot_sem, row_sem = refs[GROUP + 1 :]
    tokens = hidden.shape[1]

    def fetch(k):
        return pltpu.make_async_copy(
            blocks[k], cot_ref.at[pl.ds(k * tokens, tokens)], cot_sem.at[k]
        )

    def fetch_rows(k):
        return pltpu.make_async_copy(
            hidden.at[order_ref[k]], rows_ref.at[pl.ds(k * tokens, tokens)], row_sem.at[k]
        )

    for k in range(GROUP):
        fetch(k).start()
        fetch_rows(k).start()
    total = None
    for k in range(GROUP):
        fetch(k).wait()
        fetch_rows(k).wait()
        span = slice(k * tokens, (k + 1) * tokens)
        value = lax.dot_general(
            cot_ref[span], rows_ref[span], (((0,), (0,)), ((), ())), preferred_element_type=F32
        )
        total = value if total is None else total + value
    out_ref[...] = total.astype(BF16).reshape(out_ref.shape)


def grad_of(order, blocks, hidden, n_rep):
    tokens, depth = blocks[0].shape
    block = hidden.shape[2]
    return call(
        grad_body,
        jax.ShapeDtypeStruct((n_rep, depth // n_rep, block), BF16),
        flops=2 * GROUP * tokens * depth * block,
        limit=62,
        in_specs=[pl.BlockSpec(memory_space=pltpu.SMEM)]
        + [pl.BlockSpec(memory_space=pl.ANY)] * (GROUP + 1),
        out_specs=pl.BlockSpec(memory_space=pltpu.VMEM),
        scratch_shapes=[
            pltpu.VMEM((GROUP * tokens, depth), BF16),
            pltpu.VMEM((GROUP * tokens, block), BF16),
            pltpu.SemaphoreType.DMA((GROUP,)),
            pltpu.SemaphoreType.DMA((GROUP,)),
        ],
    )(order, *blocks, hidden)


def keep_body(taps_ref, out_ref):
    out_ref[...] = taps_ref[...]


def share_body(scale, parts_ref, taps_ref, grad_ref, small_ref):
    block = parts_ref.shape[2]
    copies, rows, width = small_ref.shape
    for zl in range(2):
        for yl in range(2):
            total = None
            for zh in range(4):
                for yh in range(4):
                    part = parts_ref[((zh * 2 + zl) * 4 + yh) * 2 + yl].astype(F32)
                    total = part if total is None else total + part
            start = (zl * 2 + yl) * block
            size = min(block, width - start)
            grad_ref[:, start : start + size] = total[:, :size] * scale
    value = grad_ref[...]
    norm = jnp.sum(value * value, axis=0, keepdims=True)
    row = lax.broadcasted_iota(jnp.int32, (rows, width), 0)
    small = jnp.where(row == rows - 1, norm, taps_ref[...]).astype(BF16)
    for k in range(copies):
        small_ref[k] = small


def chain_body(rows, *refs):
    *terms, gate_ref, up_ref, before_ref, after_ref, gate_taps, up_taps = refs[:10]
    gate_out, up_out, taps_out, gate_held, up_held, gate_back, up_back = refs[10:]
    reach = terms[0].shape[0]
    for at in range(0, gate_ref.shape[1], LANE):
        lanes = slice(at, at + LANE)

        def conv(which, source, taps, held):
            held[PAD - HALO : PAD] = before_ref[which, :, lanes].astype(F32)
            held[PAD : PAD + rows] = source[:, lanes].astype(F32)
            held[PAD + rows : PAD + rows + HALO] = after_ref[which, :, lanes].astype(F32)
            coef = [taps[k : k + 1, lanes].astype(F32) for k in range(3)]
            total = coef[2] * held[PAD : PAD + reach]
            for k in range(2):
                total += coef[k] * held[PAD - HALO + k : PAD - HALO + k + reach]
            return total, coef

        gate, gate_coef = conv(0, gate_ref, gate_taps, gate_held)
        up, up_coef = conv(1, up_ref, up_taps, up_held)
        d_hidden = terms[0][:, lanes].astype(F32)
        for term in terms[1:]:
            d_hidden += term[:, lanes].astype(F32)
        sig = 1.0 / (1.0 + jnp.exp(-gate))
        gate_back[...] = d_hidden * up * sig * (1.0 + gate * (1.0 - sig))
        up_back[...] = d_hidden * gate * sig

        def back(coef, held, out):
            total = coef[2] * held[:rows]
            for k in range(2):
                total += coef[k] * held[2 - k : 2 - k + rows]
            out[:, lanes] = total.astype(BF16)

        back(gate_coef, gate_back, gate_out)
        back(up_coef, up_back, up_out)
        for first, held, source in ((0, gate_back, gate_held), (3, up_back, up_held)):
            for k in range(3):
                start = PAD - HALO + k
                product = held[:rows] * source[start : start + rows]
                taps_out[first + k : first + k + 1, lanes] = jnp.sum(product, 0, keepdims=True)
        taps_out[6:, lanes] = jnp.zeros((2, LANE), F32)


def chain_of(terms, gate_pre, up_pre, before, after, gate_taps, up_taps, block):
    rows, width = gate_pre.shape
    reach = terms[0].shape[0]
    tall = pl.BlockSpec((reach, block), lambda i: (0, i))
    wide = pl.BlockSpec((rows, block), lambda i: (0, i))
    edge = pl.BlockSpec((2, HALO, block), lambda i: (0, 0, i))
    taps = pl.BlockSpec((3, block), lambda i: (0, i))
    grad = jax.ShapeDtypeStruct((rows, width), BF16)
    return call(
        functools.partial(chain_body, rows),
        (grad, grad, jax.ShapeDtypeStruct((8, width), F32)),
        flops=100 * rows * width,
        limit=62,
        grid=(GROUP,),
        in_specs=[tall] * 4 + [wide, wide, edge, edge, taps, taps],
        out_specs=(wide, wide, pl.BlockSpec((8, block), lambda i: (0, i))),
        scratch_shapes=[pltpu.VMEM((reach + PAD, LANE), F32)] * 2
        + [pltpu.VMEM((reach, LANE), F32)] * 2,
    )(*terms, gate_pre, up_pre, before, after, gate_taps, up_taps)


def total_of(seen_ref):
    total = None
    for source in range(seen_ref.shape[0]):
        part = seen_ref[source].astype(F32)
        total = part if total is None else total + part
    return total


def middle_body(seen_ref, small_ref):
    total = total_of(seen_ref).astype(BF16)
    for k in range(small_ref.shape[0]):
        small_ref[k] = total


def last_body(scale, seen_ref, gate_ref, up_ref, norm_ref):
    total = total_of(seen_ref)
    gate_ref[...] = total[:3] * scale
    up_ref[...] = total[3:6] * scale
    norm_ref[...] = total[7] / D


def local(gate_pre, up_pre, gate_taps, up_taps, down_weight, cotangent):
    rows, width = gate_pre.shape
    n_fs = lax.axis_size("fs")
    n_rep = lax.axis_size(ZY)
    n_near = lax.axis_size(NEAR)
    n_far = lax.axis_size(FAR)
    block = -(-(width // LANE) // GROUP) * LANE
    grad_scale = float(rows * n_rep * n_fs) ** (-0.5)

    before = passed_along(jnp.stack([gate_pre[-HALO:], up_pre[-HALO:]]), "fs", 1)
    after = passed_along(jnp.stack([gate_pre[:HALO], up_pre[:HALO]]), "fs", -1)

    def collected(flip_z, flip_y):
        pairs = []
        for z in range(8):
            for y in range(8):
                for tp in range(2):
                    to_z = mate(z, tp) if flip_z else z
                    to_y = mate(y, tp) if flip_y else y
                    pairs.append(((z * 8 + y) * 2 + tp, (to_z * 8 + to_y) * 2 + tp))
        return lax.ppermute(cotangent, ZY + ("tp",), pairs)

    blocks = [cotangent, collected(True, False)]
    blocks.append(collected(False, True))
    blocks.append(collected(True, True))
    member = lax.axis_index("zl") * 2 + lax.axis_index("yl")
    order = order_of(jnp.stack([member, member ^ 2, member ^ 1, member ^ 3]))

    hidden = hidden_of(gate_pre, up_pre, before, gate_taps, up_taps, block, n_fs)
    everyone = lax.all_to_all(
        hidden.reshape(n_near, rows, block),
        TOK + ("tp",),
        0,
        0,
        tiled=True,
        axis_index_groups=groups_of(n_fs),
    )

    me = lax.axis_index("fs")
    steps = (1, 3, 2, 0)
    hidden, cot_late = lax.optimization_barrier((hidden, cotangent))
    at = jnp.stack([(me + step) % n_fs for step in steps])
    terms = list(terms_of(at, cot_late, down_weight, rows))
    for k, step in enumerate(steps[:3]):
        pairs = [(i, (i + step) % n_fs) for i in range(n_fs)]
        terms[k] = lax.ppermute(terms[k], "fs", pairs)

    partial = grad_of(order, blocks, everyone.reshape(GROUP, -1, block), n_rep)
    parts = swap(partial, ZY)

    grad_gate, grad_up, taps = chain_of(
        terms, gate_pre, up_pre, before, after, gate_taps, up_taps, block
    )

    wide = jax.ShapeDtypeStruct((8, width), F32)
    taps = call(keep_body, wide)(taps)
    sent = functools.partial(jax.ShapeDtypeStruct, dtype=BF16)
    grad_share, small = call(
        functools.partial(share_body, grad_scale), (wide, sent((n_near, 8, width)))
    )(parts, taps)
    small = call(middle_body, sent((n_far, 8, width)))(swap(small, NEAR))
    three = jax.ShapeDtypeStruct((3, width), F32)
    gate_out, up_out, norms = call(
        functools.partial(last_body, grad_scale),
        (three, three, jax.ShapeDtypeStruct((width,), F32)),
    )(swap(small, FAR))
    return grad_gate, grad_up, gate_out, up_out, grad_share[None], norms


def solution(mesh):
    finer = Mesh(
        mesh.devices.reshape(4, 2, 4, 2, mesh.shape["fs"], mesh.shape["tp"]),
        ("zh", "zl", "yh", "yl", "fs", "tp"),
    )
    in_specs = (P(TOK, "tp"), P(TOK, "tp"), P(None, "tp"), P(None, "tp"), P("tp", "fs"), P(ZY, "fs"))
    out_specs = (P(TOK, "tp"), P(TOK, "tp"), P(None, "tp"), P(None, "tp"), P("fs", ZY, "tp"), P("tp"))
    return jax.shard_map(local, mesh=finer, in_specs=in_specs, out_specs=out_specs, check_vma=False)
```
